32 devices in a mesh: kv: 16 (over z, y, core), tp: 2 (over x).
Axes of the slice: x: 2, y: 2, z: 4, core: 2. Of those that a mesh axis runs over, the one named last changes fastest.
Arguments:
- queries: bfloat16 [4096, 1536], P('kv', 'tp'), may hold values from -6 to 6
- keys: bfloat16 [4096, 256], P('kv', 'tp'), may hold values from -6 to 6
- values: bfloat16 [4096, 256], P('kv', 'tp'), may hold values from -6 to 6
- log_sums: float32 [12, 4096], P('tp', 'kv'), may hold values from 6 to 7.5
- out_grad: bfloat16 [4096, 1536], P('kv', 'tp'), may hold values from -6 to 6
- chosen: int32 [64, 2, 8], P('kv', 'tp'), may hold values from 0 to 63, as said below
- inputs: bfloat16 [4096, 3072], P('kv', 'tp'), may hold values from -6 to 6
Outputs:
- query_grad: bfloat16 [4096, 1536], P('kv', 'tp')
- key_grad: bfloat16 [4096, 256], P('kv', 'tp')
- value_grad: bfloat16 [4096, 256], P('kv', 'tp')
- weight_grad: float32 [3072, 256], P('kv', 'tp')
The draws below stay inside these ranges and needn't reach their ends.
Inputs may be any that keep to these rules, and one draw needn't show every extreme that they name: `chosen`: for query block g and key head h, every slot holds g (an empty slot) or a key block c with g - 16 <= c < g; the blocks of the live slots of one list are distinct; each list has between 4 and 8 live slots, except that query block g has at most g of them (block 0 has none).
All inputs are finite; a program needn't handle non-finite values.
Results may differ from the reference program's by a relative error of at most 0.0049.
Values may be sent and summed in bfloat16 or wider, within the bound.
No kernel may reach another device: no remote copies, remote signals or barrier semaphores. Data moves between devices by JAX's collectives and lax.ppermute only.
A program may use at most 64 MiB of HBM per device.

```python
import jax
import jax.numpy as jnp
from jax import lax

D = 3072
HDIM = 128
QPK = 6
BLK = 64
SEL = 8
REACH = 4
BPD = 4
KVH = 2
HEADS = 12
NBLK = 64
TOKENS = 4096


def draw_chosen(key, part):
    window_span = REACH * BPD
    order_key = jax.random.fold_in(key, 11)
    count_key = jax.random.fold_in(key, 12)
    blocks = jnp.arange(NBLK, dtype=jnp.int32)[:, None, None]
    offsets = jnp.arange(1, window_span + 1, dtype=jnp.int32)[None, None, :]
    scores = jax.random.randint(order_key, (NBLK, KVH, window_span), 0, 1 << 20, dtype=jnp.int32) * window_span + offsets - 1
    scores = jnp.where(blocks - offsets >= 0, scores, -offsets)
    top_values, picked = lax.top_k(scores, SEL)
    chosen_ids = blocks - 1 - picked.astype(jnp.int32)
    live_count = jax.random.randint(count_key, (NBLK, KVH, 1), SEL // 2, SEL + 1, dtype=jnp.int32)
    slot_index = jnp.arange(SEL, dtype=jnp.int32)[None, None, :]
    keep_mask = (slot_index < live_count) & (chosen_ids >= 0)
    return jnp.where(keep_mask, chosen_ids, blocks)


def steps_of(stream_key, shape, shards, least, largest):
    factor_of = 1.0
    for dim, parts in shards:
        steps = jax.random.uniform(jax.random.fold_in(jax.random.fold_in(stream_key, 6), dim), (parts,), jnp.float32, least / len(shards), largest / len(shards))
        factor_of = factor_of * jnp.repeat(jnp.exp(steps), shape[dim] // parts).reshape((-1,) + (1,) * (len(shape) - 1 - dim))
    return factor_of


def gaussian(stream_key, shape, width, reach, split=(), kind=jnp.bfloat16):
    level = steps_of(stream_key, shape, split, -0.22, 0.18) if split else 1.0
    entries = jax.random.normal(stream_key, shape, jnp.float32) * width * level
    return jnp.minimum(jnp.maximum(entries, -reach), reach).astype(kind)


def setup_inputs(seed: int = 0) -> dict:
    splits = jax.random.split(jax.random.key(seed), 8)
    queries = gaussian(splits[0], (TOKENS, HEADS * HDIM), 1.0, 6.0, ((0, 16), (1, 2)))
    keys = gaussian(splits[1], (TOKENS, KVH * HDIM), 1.0, 6.0, ((0, 16), (1, 2)))
    values = gaussian(splits[2], (TOKENS, KVH * HDIM), 1.0, 6.0, ((0, 16), (1, 2)))
    log_sums = jnp.clip(6.0 + 1.5 * jax.random.uniform(splits[3], (HEADS, TOKENS), jnp.float32) ** steps_of(splits[3], (HEADS, TOKENS), ((0, 2), (1, 16)), -0.2, 0.2), 6.0, 7.5)
    out_grad = gaussian(splits[4], (TOKENS, HEADS * HDIM), 1.0, 6.0, ((0, 16), (1, 2)))
    chosen = draw_chosen(jax.random.fold_in(splits[7], 71), 0)
    inputs = gaussian(splits[6], (TOKENS, D), 1.0, 6.0, ((0, 16), (1, 2)))
    return {"queries": queries, "keys": keys, "values": values, "log_sums": log_sums, "out_grad": out_grad, "chosen": chosen, "inputs": inputs}


def rounded(tensor):
    return lax.optimization_barrier(tensor.astype(jnp.bfloat16)).astype(jnp.float32)


def reference(queries, keys, values, log_sums, out_grad, chosen, inputs):
    scaling = HDIM ** -0.5
    query_tile_set = queries.reshape(NBLK, BLK, KVH, QPK, HDIM)
    gradient_tiles = out_grad.reshape(NBLK, BLK, KVH, QPK, HDIM)
    sum_tiles = log_sums.reshape(KVH, QPK, NBLK, BLK).transpose(2, 0, 1, 3)
    key_tiles = keys.reshape(NBLK, BLK, KVH, HDIM)
    value_tiles = values.reshape(NBLK, BLK, KVH, HDIM)
    head_ids = jnp.arange(KVH, dtype=jnp.int32)[:, None]
    offsets = jnp.arange(BLK, dtype=jnp.int32)
    causal = (offsets[None, :] <= offsets[:, None])[None, :, None, :]

    def visit(carry, index):
        key_acc, value_acc = carry
        listed = chosen[index]
        live_slots = listed < index
        sel_keys = key_tiles[listed, :, head_ids]
        sel_values = value_tiles[listed, :, head_ids]
        own_keys = lax.dynamic_index_in_dim(key_tiles, index, 0, keepdims=False).transpose(1, 0, 2)[:, None]
        own_values = lax.dynamic_index_in_dim(value_tiles, index, 0, keepdims=False).transpose(1, 0, 2)[:, None]
        all_keys = jnp.concatenate([sel_keys, own_keys], 1).reshape(KVH, (SEL + 1) * BLK, HDIM).astype(jnp.float32)
        all_values = jnp.concatenate([sel_values, own_values], 1).reshape(KVH, (SEL + 1) * BLK, HDIM).astype(jnp.float32)
        mask_sel = jnp.broadcast_to(live_slots[:, None, :, None], (KVH, BLK, SEL, BLK))
        mask_own = jnp.broadcast_to(causal, (KVH, BLK, 1, BLK))
        permitted_mask = jnp.concatenate([mask_sel, mask_own], 2).reshape(KVH, BLK, (SEL + 1) * BLK)
        query_rows = lax.dynamic_index_in_dim(query_tile_set, index, 0, keepdims=False).astype(jnp.float32)
        grad_rows = lax.dynamic_index_in_dim(gradient_tiles, index, 0, keepdims=False).astype(jnp.float32)
        sum_rows = lax.dynamic_index_in_dim(sum_tiles, index, 0, keepdims=False)
        scores = jnp.einsum('qhgd,hkd->hgqk', query_rows, all_keys) * scaling
        weights = jnp.where(permitted_mask[:, None], jnp.exp(scores - sum_rows[..., None]), 0.0)
        grad_weights = jnp.einsum('qhgd,hkd->hgqk', grad_rows, all_values)
        delta_rows = jnp.sum(weights * grad_weights, -1, keepdims=True)
        score_gradient = rounded(weights * (grad_weights - delta_rows))
        weights_reduced = rounded(weights)
        query_part = jnp.einsum('hgqk,hkd->qhgd', score_gradient, all_keys) * scaling
        key_part = (jnp.einsum('hgqk,qhgd->hkd', score_gradient, query_rows) * scaling).reshape(KVH, SEL + 1, BLK, HDIM)
        value_part = jnp.einsum('hgqk,qhgd->hkd', weights_reduced, grad_rows).reshape(KVH, SEL + 1, BLK, HDIM)
        key_acc = key_acc.at[listed, :, head_ids].add(key_part[:, :SEL])
        key_acc = key_acc.at[index].add(key_part[:, SEL].transpose(1, 0, 2))
        value_acc = value_acc.at[listed, :, head_ids].add(value_part[:, :SEL])
        value_acc = value_acc.at[index].add(value_part[:, SEL].transpose(1, 0, 2))
        return (key_acc, value_acc), query_part.reshape(BLK, HEADS * HDIM).astype(jnp.bfloat16)

    zeros_acc = jnp.zeros((NBLK, BLK, KVH, HDIM), jnp.float32)
    (key_acc, value_acc), query_blocks = lax.scan(visit, (zeros_acc, zeros_acc), jnp.arange(NBLK, dtype=jnp.int32))
    query_grad = query_blocks.reshape(TOKENS, HEADS * HDIM)
    key_grad = key_acc.reshape(TOKENS, KVH * HDIM).astype(jnp.bfloat16)
    value_grad = value_acc.reshape(TOKENS, KVH * HDIM).astype(jnp.bfloat16)
    weight_grad = jnp.dot(inputs.T, value_grad, preferred_element_type=jnp.float32)
    return (query_grad, key_grad, value_grad, weight_grad)
```

```python
import functools

import jax
import jax.numpy as jnp
from jax import lax
from jax.experimental import pallas as pl
from jax.experimental.pallas import tpu as pltpu
from jax.sharding import PartitionSpec as P

REACH = 4
LOG2E = 1.4426950408889634


def vmem(count):
    return [pl.BlockSpec(memory_space=pltpu.VMEM)] * count


def shifted(value, steps):
    count = lax.axis_size("kv")
    return lax.ppermute(
        value, "kv", [(i, i + steps) for i in range(max(0, -steps), min(count, count - steps))]
    )


def swapped(value, bit):
    count = lax.axis_size("kv")
    return lax.ppermute(value, "kv", [(i, i ^ bit) for i in range(count)])


def turned(value, stride, radix, steps):
    count = lax.axis_size("kv")
    pairs = []
    for i in range(count):
        digit = i // stride % radix
        pairs.append((i, i + ((digit + steps) % radix - digit) * stride))
    return lax.ppermute(value, "kv", pairs)


def attention_kernel(
    block,
    heads,
    chosen_ref,
    queries_ref,
    out_grad_ref,
    sums_ref,
    own_ref,
    two_ref,
    four_ref,
    peer_ref,
    peer_two_ref,
    peer_four_ref,
    query_grad_ref,
    value_mine_ref,
    value_peer_ref,
    key_mine_ref,
    key_peer_ref,
    window,
    key_acc,
    value_acc,
    key_rows,
    value_rows,
):
    width = queries_ref.shape[1] // heads
    tokens = queries_ref.shape[0]
    blocks = tokens // block
    slots = chosen_ref.shape[2]
    scaling = width ** (-0.5)
    device = lax.axis_index("kv")
    odd = lax.rem(device, 2)

    def place(position, ref):
        for b in range(blocks):
            window[position * blocks + b] = ref[pl.ds(b * block, block), :]

    place(4, own_ref)
    place(2, two_ref)
    place(0, four_ref)

    @pl.when(odd == 0)
    def _():
        place(3, peer_two_ref)
        place(1, peer_four_ref)

    @pl.when(odd == 1)
    def _():
        place(3, peer_ref)
        place(1, peer_two_ref)

    key_acc[...] = jnp.zeros_like(key_acc)
    value_acc[...] = jnp.zeros_like(value_acc)
    first = (device - REACH) * blocks
    rows = heads * block
    key_pos = lax.broadcasted_iota(jnp.int32, (block, rows), 0)
    query_pos = lax.rem(lax.broadcasted_iota(jnp.int32, (block, rows), 1), block)
    causal = key_pos <= query_pos
    for b in range(blocks):
        here = pl.ds(b * block, block)
        places = []
        offsets = []
        for s in range(slots):
            listed = chosen_ref[b, 0, s]
            places.append(listed - first)
            live = listed < device * blocks + b
            offsets.append(jnp.where(live, 0.0, 1e30))
        places.append(REACH * blocks + b)
        offsets.append(0.0)
        for s in range(slots + 1):
            key_rows[pl.ds(s * block, block), :] = window[places[s], :, :width]
            value_rows[pl.ds(s * block, block), :] = window[places[s], :, width:]
        q = jnp.concatenate(
            [queries_ref[here, pl.ds(a * width, width)] for a in range(heads)], 0
        )
        g = jnp.concatenate(
            [out_grad_ref[here, pl.ds(a * width, width)] for a in range(heads)], 0
        )
        sums = jnp.concatenate([sums_ref[pl.ds(a, 1), here] for a in range(heads)], 1) * LOG2E
        keys = key_rows[...]
        scores = lax.dot_general(
            keys, q, (((1,), (1,)), ((), ())), preferred_element_type=jnp.float32
        )
        grads = lax.dot_general(
            value_rows[...], g, (((1,), (1,)), ((), ())), preferred_element_type=jnp.float32
        )
        weights = []
        delta = jnp.zeros((1, rows), jnp.float32)
        for s in range(slots + 1):
            part = slice(s * block, (s + 1) * block)
            weight = jnp.exp2(scores[part] * (scaling * LOG2E) - (sums + offsets[s]))
            if s == slots:
                weight = jnp.where(causal, weight, 0.0)
            weights.append(weight)
            delta = delta + jnp.sum(weight * grads[part], 0, keepdims=True)
        score_grads = jnp.concatenate(
            [
                (weights[s] * (grads[s * block : (s + 1) * block] - delta)).astype(jnp.bfloat16)
                for s in range(slots + 1)
            ],
            0,
        )
        low = jnp.concatenate([w.astype(jnp.bfloat16) for w in weights], 0)
        value_part = jnp.dot(low, g, preferred_element_type=jnp.float32)
        key_part = jnp.dot(score_grads, q, preferred_element_type=jnp.float32) * scaling
        query_part = (
            lax.dot_general(
                score_grads, keys, (((0,), (0,)), ((), ())), preferred_element_type=jnp.float32
            )
            * scaling
        )
        for a in range(heads):
            query_grad_ref[here, pl.ds(a * width, width)] = query_part[
                a * block : (a + 1) * block
            ].astype(jnp.bfloat16)
        for s in range(slots + 1):
            key_acc[places[s]] += key_part[s * block : (s + 1) * block]
            value_acc[places[s]] += value_part[s * block : (s + 1) * block]

    for acc, mine_ref, peer_out in (
        (value_acc, value_mine_ref, value_peer_ref),
        (key_acc, key_mine_ref, key_peer_ref),
    ):
        for slot, position in enumerate((4, 2, 0)):
            for b in range(blocks):
                mine_ref[slot, pl.ds(b * block, block), :] = acc[position * blocks + b]

        def give(slot, position, acc=acc, peer_out=peer_out):
            for b in range(blocks):
                if position is None:
                    piece = jnp.zeros((block, width), jnp.bfloat16)
                else:
                    piece = acc[position * blocks + b].astype(jnp.bfloat16)
                peer_out[slot, pl.ds(b * block, block), :] = piece

        @pl.when(odd == 0)
        def _(give=give):
            give(0, None)
            give(1, 3)
            give(2, 1)

        @pl.when(odd == 1)
        def _(give=give):
            give(0, 3)
            give(1, 1)
            give(2, None)


def transpose_kernel(piece, inputs_ref, keep_ref, send_ref, turned_rows):
    turned_rows[...] = inputs_ref[...].T
    odd = lax.rem(lax.axis_index("kv"), 2)
    for pair in range(keep_ref.shape[0] // piece):
        here = pl.ds(pair * piece, piece)
        keep_ref[here, :] = turned_rows[pl.ds((2 * pair + odd) * piece, piece), :]
        send_ref[here, :] = turned_rows[pl.ds((2 * pair + 1 - odd) * piece, piece), :]


def product_kernel(piece, shares, *refs):
    mine_ref, peer_ref = refs[:2]
    factors = refs[2 : 2 + 2 * shares]
    keep_ref, send_ref = refs[2 + 2 * shares : 4 + 2 * shares]
    result = refs[4 + 2 * shares]
    part = lax.axis_index("tp")
    bit = lax.rem(lax.axis_index("kv") // 2, 2)
    per_share = factors[0].shape[0] // piece
    for step in range(shares):
        own, other = factors[2 * step], factors[2 * step + 1]
        where = lax.rem(part + shares - step, shares)
        total = jnp.dot(own[...], mine_ref[...], preferred_element_type=jnp.float32)
        total += jnp.dot(other[...], peer_ref[...], preferred_element_type=jnp.float32)
        for i in range(per_share):
            result[where * per_share + i] = total[i * piece : (i + 1) * piece]
    for i in range(keep_ref.shape[0]):
        keep_ref[i] = result[2 * i + bit]
        send_ref[i] = result[2 * i + 1 - bit].astype(jnp.bfloat16)


def spread_kernel(stride, radix, keep_ref, came_ref, *outs):
    mine_ref, sends = outs[0], outs[1:]
    digit = lax.rem(lax.axis_index("kv") // stride, radix)
    for i in range(mine_ref.shape[0]):
        at = radix * i + digit
        mine_ref[i] = keep_ref[at] + came_ref[at].astype(jnp.float32)
        for s, send in enumerate(sends):
            at = radix * i + lax.rem(digit + s + 1, radix)
            send[i] = (keep_ref[at] + came_ref[at].astype(jnp.float32)).astype(jnp.bfloat16)


def spread(kept, came, stride, radix):
    shape = (kept.shape[0] // radix,) + kept.shape[1:]
    outs = [jax.ShapeDtypeStruct(shape, jnp.float32)]
    outs += [jax.ShapeDtypeStruct(shape, jnp.bfloat16)] * (radix - 1)
    return pl.pallas_call(
        functools.partial(spread_kernel, stride, radix),
        out_shape=outs,
        in_specs=vmem(2),
        out_specs=vmem(radix),
    )(kept, came)


def radices(count):
    found = []
    for radix in (4, 3, 2):
        while count % radix == 0:
            found.append(radix)
            count //= radix
    if count > 1:
        found.append(count)
    return found


def shards(queries, keys, values, log_sums, out_grad, chosen, inputs):
    tokens, width = keys.shape
    blocks = chosen.shape[0]
    block = tokens // blocks
    heads = queries.shape[1] // width
    slots = chosen.shape[2]
    count = lax.axis_size("kv")
    shares = lax.axis_size("tp")
    features = inputs.shape[1]
    piece = features * shares // count
    bf16, f32 = jnp.bfloat16, jnp.float32

    pair = jnp.concatenate([keys, values], 1)
    two = shifted(pair, 2)
    four = shifted(pair, 4)
    peer = swapped(pair, 1)
    peer_two = swapped(two, 1)
    peer_four = swapped(four, 1)

    keep, send = pl.pallas_call(
        functools.partial(transpose_kernel, piece),
        out_shape=[jax.ShapeDtypeStruct((features // 2, tokens), bf16)] * 2,
        in_specs=vmem(1),
        out_specs=vmem(2),
        scratch_shapes=[pltpu.VMEM((features, tokens), bf16)],
    )(inputs)
    other = swapped(send, 1)
    factors = [keep, other]
    for step in range(1, shares):
        pairs = [(i, (i + step) % shares) for i in range(shares)]
        factors += [lax.ppermute(keep, "tp", pairs), lax.ppermute(other, "tp", pairs)]

    query_grad, value_mine, value_peer, key_mine, key_peer = pl.pallas_call(
        functools.partial(attention_kernel, block, heads),
        out_shape=[
            jax.ShapeDtypeStruct(queries.shape, bf16),
            jax.ShapeDtypeStruct((3, tokens, width), f32),
            jax.ShapeDtypeStruct((3, tokens, width), bf16),
            jax.ShapeDtypeStruct((3, tokens, width), f32),
            jax.ShapeDtypeStruct((3, tokens, width), bf16),
        ],
        in_specs=[pl.BlockSpec(memory_space=pltpu.SMEM)] + vmem(9),
        out_specs=vmem(5),
        scratch_shapes=[
            pltpu.VMEM(((REACH + 1) * blocks, block, 2 * width), bf16),
            pltpu.VMEM(((REACH + 1) * blocks, block, width), f32),
            pltpu.VMEM(((REACH + 1) * blocks, block, width), f32),
            pltpu.VMEM(((slots + 1) * block, width), bf16),
            pltpu.VMEM(((slots + 1) * block, width), bf16),
        ],
    )(chosen, queries, out_grad, log_sums, pair, two, four, peer, peer_two, peer_four)

    def gathered(mine, peer_part):
        came = swapped(peer_part, 1).astype(f32)
        back_two = shifted((mine[1] + came[1]).astype(bf16), -2)
        back_four = shifted((mine[2] + came[2]).astype(bf16), -4)
        total = mine[0] + came[0] + back_two.astype(f32) + back_four.astype(f32)
        return total.astype(bf16)

    value_grad = gathered(value_mine, value_peer)
    value_other = swapped(value_grad, 1)
    key_grad = gathered(key_mine, key_peer)

    pieces = count // 4
    kept, sent = pl.pallas_call(
        functools.partial(product_kernel, piece, shares),
        out_shape=[
            jax.ShapeDtypeStruct((pieces, piece, width), f32),
            jax.ShapeDtypeStruct((pieces, piece, width), bf16),
        ],
        in_specs=vmem(2 + 2 * shares),
        out_specs=vmem(2),
        scratch_shapes=[pltpu.VMEM((2 * pieces, piece, width), f32)],
    )(value_grad, value_other, *factors)
    came = swapped(sent, 2)
    stride = 4
    for radix in radices(pieces):
        kept, *sends = spread(kept, came, stride, radix)
        came = sum(turned(v, stride, radix, s + 1).astype(f32) for s, v in enumerate(sends))
        stride *= radix
    weight_grad = (kept + came)[0]
    return (query_grad, key_grad, value_grad, weight_grad)


def solution(mesh):
    in_specs = (
        P("kv", "tp"),
        P("kv", "tp"),
        P("kv", "tp"),
        P("tp", "kv"),
        P("kv", "tp"),
        P("kv", "tp", None),
        P("kv", "tp"),
    )
    out_specs = (P("kv", "tp"), P("kv", "tp"), P("kv", "tp"), P("kv", "tp"))
    return jax.shard_map(shards, mesh=mesh, in_specs=in_specs, out_specs=out_specs, check_vma=False)
```

```python
import functools

import jax
import jax.numpy as jnp
from jax import lax
from jax.experimental import pallas as pl
from jax.experimental.pallas import tpu as pltpu
from jax.sharding import PartitionSpec as P


REACH = 4
LOG2E = 1.4426950408889634


PARAMS = pltpu.CompilerParams(vmem_limit_bytes=24 << 20)


def vmem(count):
    return [pl.BlockSpec(memory_space=pltpu.VMEM)] * count


def near(*values):
    return [pltpu.with_memory_space_constraint(v, pltpu.VMEM) for v in values]


def shifted(value, steps):
    count = lax.axis_size("kv")
    return lax.ppermute(
        value, "kv", [(i, i + steps) for i in range(max(0, -steps), min(count, count - steps))]
    )


def returned(value):
    count = lax.axis_size("kv")
    moves = [(i, i - (4 if i % 2 else 2)) for i in range(count)]
    return lax.ppermute(value, "kv", [m for m in moves if m[1] >= 0])


def swapped(value, bit):
    count = lax.axis_size("kv")
    return lax.ppermute(value, "kv", [(i, i ^ bit) for i in range(count)])


def turned(value, stride, radix, steps):
    count = lax.axis_size("kv")
    pairs = []
    for i in range(count):
        digit = i // stride % radix
        target = (digit + steps) % radix if radix & (radix - 1) else digit ^ steps
        pairs.append((i, i + (target - digit) * stride))
    return lax.ppermute(value, "kv", pairs)


def attention_kernel(
    block,
    heads,
    chosen_ref,
    queries_ref,
    out_grad_ref,
    sums_ref,
    own_ref,
    two_ref,
    four_ref,
    peer_ref,
    peer_two_ref,
    peer_four_ref,
    query_grad_ref,
    value_acc,
    value_low_ref,
    key_acc,
    key_low_ref,
    window,
    key_rows,
    value_rows,
):
    width = queries_ref.shape[1] // heads
    tokens = queries_ref.shape[0]
    blocks = tokens // block
    slots = chosen_ref.shape[2]
    scaling = width ** (-0.5)
    device = lax.axis_index("kv")
    odd = lax.rem(device, 2)

    def place(position, ref):
        for b in range(blocks):
            window[position * blocks + b] = ref[pl.ds(b * block, block), :]

    for back, (mine, theirs) in enumerate(
        ((own_ref, peer_ref), (two_ref, peer_two_ref), (four_ref, peer_four_ref))
    ):
        place(REACH - 2 * back + odd, mine)
        place(REACH - 2 * back + 1 - odd, theirs)

    key_acc[...] = jnp.zeros_like(key_acc)
    value_acc[...] = jnp.zeros_like(value_acc)
    first = (device - odd - REACH) * blocks
    rows = heads * block
    key_pos = lax.broadcasted_iota(jnp.int32, (block, rows), 0)
    query_pos = lax.rem(lax.broadcasted_iota(jnp.int32, (block, rows), 1), block)
    causal = key_pos <= query_pos
    for b in range(blocks):
        here = pl.ds(b * block, block)
        places = []
        offsets = []
        for s in range(slots):
            listed = chosen_ref[b, 0, s]
            places.append(listed - first)
            live = listed < device * blocks + b
            offsets.append(jnp.where(live, 0.0, 1e30))
        places.append((REACH + odd) * blocks + b)
        offsets.append(0.0)
        for s in range(slots + 1):
            key_rows[pl.ds(s * block, block), :] = window[places[s], :, :width]
            value_rows[pl.ds(s * block, block), :] = window[places[s], :, width:]
        q = jnp.concatenate(
            [queries_ref[here, pl.ds(a * width, width)] for a in range(heads)], 0
        )
        g = jnp.concatenate(
            [out_grad_ref[here, pl.ds(a * width, width)] for a in range(heads)], 0
        )
        sums = jnp.concatenate([sums_ref[pl.ds(a, 1), here] for a in range(heads)], 1) * LOG2E
        keys = key_rows[...]
        scores = lax.dot_general(
            keys, q, (((1,), (1,)), ((), ())), preferred_element_type=jnp.float32
        )
        grads = lax.dot_general(
            value_rows[...], g, (((1,), (1,)), ((), ())), preferred_element_type=jnp.float32
        )
        weights = []
        delta = jnp.zeros((1, rows), jnp.float32)
        for s in range(slots + 1):
            part = slice(s * block, (s + 1) * block)
            weight = jnp.exp2(scores[part] * (scaling * LOG2E) - (sums + offsets[s]))
            if s == slots:
                weight = jnp.where(causal, weight, 0.0)
            weights.append(weight)
            delta = delta + jnp.sum(weight * grads[part], 0, keepdims=True)
        score_grads = jnp.concatenate(
            [
                (weights[s] * (grads[s * block : (s + 1) * block] - delta)).astype(jnp.bfloat16)
                for s in range(slots + 1)
            ],
            0,
        )
        low = jnp.concatenate([w.astype(jnp.bfloat16) for w in weights], 0)
        value_part = jnp.dot(low, g, preferred_element_type=jnp.float32)
        key_part = jnp.dot(score_grads, q, preferred_element_type=jnp.float32) * scaling
        query_part = (
            lax.dot_general(
                score_grads, keys, (((0,), (0,)), ((), ())), preferred_element_type=jnp.float32
            )
            * scaling
        )
        for a in range(heads):
            query_grad_ref[here, pl.ds(a * width, width)] = query_part[
                a * block : (a + 1) * block
            ].astype(jnp.bfloat16)
        for s in range(slots + 1):
            key_acc[places[s]] += key_part[s * block : (s + 1) * block]
            value_acc[places[s]] += value_part[s * block : (s + 1) * block]

    value_low_ref[...] = value_acc[...].astype(jnp.bfloat16)
    key_low_ref[...] = key_acc[...].astype(jnp.bfloat16)


def chip_sum_kernel(mine_ref, came_ref, own_ref, send_ref):
    half = own_ref.shape[0]
    odd = lax.rem(lax.axis_index("kv"), 2)
    last = mine_ref.shape[0] - half
    own_ref[...] = mine_ref[pl.ds(last, half)] + came_ref[pl.ds(last, half)].astype(jnp.float32)
    at = (1 - odd) * half
    total = mine_ref[pl.ds(at, half)] + came_ref[pl.ds(at, half)].astype(jnp.float32)
    send_ref[...] = total.astype(jnp.bfloat16)


def total_kernel(own_ref, back_ref, other_ref, both_ref, grad_ref):
    total = own_ref[...] + back_ref[...].astype(jnp.float32) + other_ref[...].astype(jnp.float32)
    both_ref[...] = total.reshape(both_ref.shape).astype(jnp.bfloat16)
    tokens = grad_ref.shape[0]
    odd = lax.rem(lax.axis_index("kv"), 2)
    grad_ref[...] = both_ref[pl.ds(pl.multiple_of(odd * tokens, tokens), tokens), :]


def prepare_kernel(piece, keys_ref, values_ref, inputs_ref, pair_ref, keep_ref, give_ref, turned_rows):
    width = keys_ref.shape[1]
    pair_ref[:, :width] = keys_ref[...]
    pair_ref[:, width:] = values_ref[...]
    turned_rows[...] = inputs_ref[...].T
    corner = lax.rem(lax.axis_index("kv"), 4)
    for i in range(2):
        for out, owner in ((keep_ref, corner ^ (2 * i)), (give_ref, corner ^ (2 * i + 1))):
            for group in range(out.shape[1] // piece):
                out[i, pl.ds(group * piece, piece), :] = turned_rows[
                    pl.ds((4 * group + owner) * piece, piece), :
                ]


def join_kernel(keep_ref, got_ref, own_ref, across_ref):
    tokens = keep_ref.shape[2]
    odd = lax.rem(lax.axis_index("kv"), 2)
    for i, out in enumerate((own_ref, across_ref)):
        out[:, pl.ds(pl.multiple_of(odd * tokens, tokens), tokens)] = keep_ref[i]
        out[:, pl.ds(pl.multiple_of((1 - odd) * tokens, tokens), tokens)] = got_ref[i]


def partner(digit, step, radix):
    if radix & (radix - 1):
        return lax.rem(digit + step, radix)
    return digit ^ step


def product_kernel(shares, stride, radix, *refs):
    grads, factors = refs[:2], refs[2 : 2 + 2 * shares]
    outs = refs[2 + 2 * shares :]
    mine_ref, sends, result = outs[0], outs[1:radix], outs[radix]
    piece = result.shape[1]
    part = lax.axis_index("tp")
    per_share = factors[0].shape[0] // piece
    for step in range(shares):
        where = lax.rem(part + shares - step, shares)
        total = 0.0
        for i in range(2):
            total += jnp.dot(
                factors[2 * step + i][...], grads[i][...], preferred_element_type=jnp.float32
            )
        for i in range(per_share):
            result[where * per_share + i] = total[i * piece : (i + 1) * piece]
    digit = lax.rem(lax.axis_index("kv") // stride, radix)
    for i in range(mine_ref.shape[0]):
        mine_ref[i] = result[radix * i + digit]
        for s, send in enumerate(sends):
            send[i] = result[radix * i + partner(digit, s + 1, radix)].astype(jnp.bfloat16)


def spread_kernel(stride, radix, keep_ref, came_ref, *outs):
    mine_ref, sends = outs[0], outs[1:]
    digit = lax.rem(lax.axis_index("kv") // stride, radix)
    for i in range(mine_ref.shape[0]):
        at = radix * i + digit
        mine_ref[i] = keep_ref[at] + came_ref[at].astype(jnp.float32)
        for s, send in enumerate(sends):
            at = radix * i + partner(digit, s + 1, radix)
            send[i] = (keep_ref[at] + came_ref[at].astype(jnp.float32)).astype(jnp.bfloat16)


def spread(kept, came, stride, radix):
    shape = (kept.shape[0] // radix,) + kept.shape[1:]
    outs = [jax.ShapeDtypeStruct(shape, jnp.float32)]
    outs += [jax.ShapeDtypeStruct(shape, jnp.bfloat16)] * (radix - 1)
    return pl.pallas_call(
        functools.partial(spread_kernel, stride, radix),
        out_shape=outs,
        in_specs=vmem(2),
        out_specs=vmem(radix),
    )(kept, came)


def radices(count):
    found = []
    for radix in (4, 3, 2):
        while count % radix == 0:
            found.append(radix)
            count //= radix
    if count > 1:
        found.append(count)
    return found


def shards(queries, keys, values, log_sums, out_grad, chosen, inputs):
    tokens, width = keys.shape
    blocks = chosen.shape[0]
    block = tokens // blocks
    heads = queries.shape[1] // width
    slots = chosen.shape[2]
    count = lax.axis_size("kv")
    shares = lax.axis_size("tp")
    features = inputs.shape[1]
    piece = features * shares // count
    window = (REACH + 2) * blocks
    bf16, f32 = jnp.bfloat16, jnp.float32

    pair, keep, give = pl.pallas_call(
        functools.partial(prepare_kernel, piece),
        out_shape=[pltpu.VMEM((tokens, 2 * width), bf16)]
        + [pltpu.VMEM((2, features // 4, tokens), bf16)] * 2,
        in_specs=vmem(3),
        out_specs=vmem(3),
        scratch_shapes=[pltpu.VMEM((features, tokens), bf16)],
        compiler_params=PARAMS,
    )(*near(keys, values, inputs))
    four = shifted(pair, 4)
    two = shifted(pair, 2)
    peer = swapped(pair, 1)
    peer_four = swapped(four, 1)
    peer_two = swapped(two, 1)

    got = swapped(give, 1)
    own_factor, across = pl.pallas_call(
        join_kernel,
        out_shape=[pltpu.VMEM((features // 4, 2 * tokens), bf16)] * 2,
        in_specs=vmem(2),
        out_specs=vmem(2),
        compiler_params=PARAMS,
    )(*near(keep, got))
    side_factor = swapped(across, 2)
    factors = [own_factor, side_factor]
    for step in range(1, shares):
        pairs = [(i, (i + step) % shares) for i in range(shares)]
        for i in range(2):
            factors.append(lax.ppermute(factors[i], "tp", pairs))

    query_grad, value_acc, value_low, key_acc, key_low = pl.pallas_call(
        functools.partial(attention_kernel, block, heads),
        out_shape=[
            jax.ShapeDtypeStruct(queries.shape, bf16),
            pltpu.VMEM((window, block, width), f32),
            pltpu.VMEM((window, block, width), bf16),
            pltpu.VMEM((window, block, width), f32),
            pltpu.VMEM((window, block, width), bf16),
        ],
        in_specs=[pl.BlockSpec(memory_space=pltpu.SMEM)] + vmem(9),
        out_specs=vmem(5),
        scratch_shapes=[
            pltpu.VMEM((window, block, 2 * width), bf16),
            pltpu.VMEM(((slots + 1) * block, width), bf16),
            pltpu.VMEM(((slots + 1) * block, width), bf16),
        ],
        compiler_params=PARAMS,
    )(
        chosen,
        *near(queries, out_grad, log_sums, pair, two, four, peer, peer_two, peer_four),
    )

    def gathered(acc, low):
        came = swapped(low, 1)
        own, send = pl.pallas_call(
            chip_sum_kernel,
            out_shape=[
                pltpu.VMEM((2 * blocks, block, width), f32),
                pltpu.VMEM((2 * blocks, block, width), bf16),
            ],
            in_specs=vmem(2),
            out_specs=vmem(2),
            compiler_params=PARAMS,
        )(*near(acc, came))
        back = returned(send)
        other = swapped(back, 1)
        return pl.pallas_call(
            total_kernel,
            out_shape=[
                pltpu.VMEM((2 * tokens, width), bf16),
                jax.ShapeDtypeStruct((tokens, width), bf16),
            ],
            in_specs=vmem(3),
            out_specs=vmem(2),
            compiler_params=PARAMS,
        )(*near(own, back, other))

    value_both, value_grad = gathered(value_acc, value_low)
    _, key_grad = gathered(key_acc, key_low)
    value_side = swapped(value_both, 2)

    pieces = count // 4
    stages = radices(pieces)
    kept, *sends = pl.pallas_call(
        functools.partial(product_kernel, shares, 4, stages[0]),
        out_shape=[pltpu.VMEM((pieces // stages[0], piece, width), f32)]
        + [pltpu.VMEM((pieces // stages[0], piece, width), bf16)] * (stages[0] - 1),
        in_specs=vmem(2 + 2 * shares),
        out_specs=vmem(stages[0]),
        scratch_shapes=[pltpu.VMEM((pieces, piece, width), f32)],
        compiler_params=PARAMS,
    )(*near(value_both, value_side, *factors))
    stride = 4
    for stage, radix in enumerate(stages):
        if stage:
            kept, *sends = spread(kept, came, stride, radix)
        came = 0.0
        for s, send in enumerate(sends):
            came = came + turned(send, stride, radix, s + 1).astype(f32)
        stride *= radix
    weight_grad = (kept + came)[0]
    return (query_grad, key_grad, value_grad, weight_grad)


def solution(mesh):
    in_specs = (
        P("kv", "tp"),
        P("kv", "tp"),
        P("kv", "tp"),
        P("tp", "kv"),
        P("kv", "tp"),
        P("kv", "tp", None),
        P("kv", "tp"),
    )
    out_specs = (P("kv", "tp"), P("kv", "tp"), P("kv", "tp"), P("kv", "tp"))

    return jax.shard_map(shards, mesh=mesh, in_specs=in_specs, out_specs=out_specs, check_vma=False)
```

```python
import functools

import jax
import jax.numpy as jnp
from jax import lax
from jax.experimental import pallas as pl
from jax.experimental.pallas import tpu as pltpu
from jax.sharding import PartitionSpec as P


REACH = 4
LOG2E = 1.4426950408889634


PARAMS = pltpu.CompilerParams(vmem_limit_bytes=24 << 20)


def vmem(count):
    return [pl.BlockSpec(memory_space=pltpu.VMEM)] * count


def near(*values):
    return [pltpu.with_memory_space_constraint(v, pltpu.VMEM) for v in values]


def shifted(value, steps):
    count = lax.axis_size("kv")
    return lax.ppermute(value, "kv", [(i, (i + steps) % count) for i in range(count)])


def returned(value):
    count = lax.axis_size("kv")
    moves = [(i, (i - (4 if i % 2 else 2)) % count) for i in range(count)]
    return lax.ppermute(value, "kv", moves)


def swapped(value, bit):
    count = lax.axis_size("kv")
    return lax.ppermute(value, "kv", [(i, i ^ bit) for i in range(count)])


def turned(value, stride, radix, steps):
    count = lax.axis_size("kv")
    pairs = []
    for i in range(count):
        digit = i // stride % radix
        target = (digit + steps) % radix if radix & (radix - 1) else digit ^ steps
        pairs.append((i, i + (target - digit) * stride))
    return lax.ppermute(value, "kv", pairs)


def attention_kernel(
    block,
    heads,
    chosen_ref,
    queries_ref,
    out_grad_ref,
    sums_ref,
    own_ref,
    two_ref,
    four_ref,
    peer_ref,
    peer_two_ref,
    peer_four_ref,
    query_grad_ref,
    value_acc,
    value_low_ref,
    key_acc,
    key_low_ref,
    window,
    key_rows,
    value_rows,
):
    width = queries_ref.shape[1] // heads
    tokens = queries_ref.shape[0]
    blocks = tokens // block
    slots = chosen_ref.shape[2]
    scaling = width ** (-0.5)
    device = lax.axis_index("kv")
    odd = lax.rem(device, 2)

    def place(position, ref):
        for b in range(blocks):
            window[position * blocks + b] = ref[pl.ds(b * block, block), :]

    for back, (mine, theirs) in enumerate(
        ((own_ref, peer_ref), (two_ref, peer_two_ref), (four_ref, peer_four_ref))
    ):
        place(REACH - 2 * back + odd, mine)
        place(REACH - 2 * back + 1 - odd, theirs)

    key_acc[...] = jnp.zeros_like(key_acc)
    value_acc[...] = jnp.zeros_like(value_acc)
    first = (device - odd - REACH) * blocks
    rows = heads * block
    key_pos = lax.broadcasted_iota(jnp.int32, (block, rows), 0)
    query_pos = lax.rem(lax.broadcasted_iota(jnp.int32, (block, rows), 1), block)
    causal = key_pos <= query_pos
    for b in range(blocks):
        here = pl.ds(b * block, block)
        places = []
        offsets = []
        for s in range(slots):
            listed = chosen_ref[b, 0, s]
            places.append(listed - first)
            live = listed < device * blocks + b
            offsets.append(jnp.where(live, 0.0, 1e30))
        places.append((REACH + odd) * blocks + b)
        offsets.append(0.0)
        for s in range(slots + 1):
            key_rows[pl.ds(s * block, block), :] = window[places[s], :, :width]
            value_rows[pl.ds(s * block, block), :] = window[places[s], :, width:]
        q = jnp.concatenate(
            [queries_ref[here, pl.ds(a * width, width)] for a in range(heads)], 0
        )
        g = jnp.concatenate(
            [out_grad_ref[here, pl.ds(a * width, width)] for a in range(heads)], 0
        )
        sums = jnp.concatenate([sums_ref[pl.ds(a, 1), here] for a in range(heads)], 1) * LOG2E
        keys = key_rows[...]
        scores = lax.dot_general(
            keys, q, (((1,), (1,)), ((), ())), preferred_element_type=jnp.float32
        )
        grads = lax.dot_general(
            value_rows[...], g, (((1,), (1,)), ((), ())), preferred_element_type=jnp.float32
        )
        weights = []
        delta = jnp.zeros((1, rows), jnp.float32)
        for s in range(slots + 1):
            part = slice(s * block, (s + 1) * block)
            weight = jnp.exp2(scores[part] * (scaling * LOG2E) - (sums + offsets[s]))
            if s == slots:
                weight = jnp.where(causal, weight, 0.0)
            weights.append(weight)
            delta = delta + jnp.sum(weight * grads[part], 0, keepdims=True)
        score_grads = jnp.concatenate(
            [
                (weights[s] * (grads[s * block : (s + 1) * block] - delta)).astype(jnp.bfloat16)
                for s in range(slots + 1)
            ],
            0,
        )
        low = jnp.concatenate([w.astype(jnp.bfloat16) for w in weights], 0)
        value_part = jnp.dot(low, g, preferred_element_type=jnp.float32)
        key_part = jnp.dot(score_grads, q, preferred_element_type=jnp.float32) * scaling
        query_part = (
            lax.dot_general(
                score_grads, keys, (((0,), (0,)), ((), ())), preferred_element_type=jnp.float32
            )
            * scaling
        )
        for a in range(heads):
            query_grad_ref[here, pl.ds(a * width, width)] = query_part[
                a * block : (a + 1) * block
            ].astype(jnp.bfloat16)
        for s in range(slots + 1):
            key_acc[places[s]] += key_part[s * block : (s + 1) * block]
            value_acc[places[s]] += value_part[s * block : (s + 1) * block]

    value_low_ref[...] = value_acc[...].astype(jnp.bfloat16)
    key_low_ref[...] = key_acc[...].astype(jnp.bfloat16)


def chip_sum_kernel(mine_ref, came_ref, own_ref, send_ref):
    half = own_ref.shape[0]
    odd = lax.rem(lax.axis_index("kv"), 2)
    last = mine_ref.shape[0] - half
    own_ref[...] = mine_ref[pl.ds(last, half)] + came_ref[pl.ds(last, half)].astype(jnp.float32)
    at = (1 - odd) * half
    total = mine_ref[pl.ds(at, half)] + came_ref[pl.ds(at, half)].astype(jnp.float32)
    send_ref[...] = total.astype(jnp.bfloat16)


def total_kernel(own_ref, back_ref, other_ref, *refs):
    grad_ref = refs[-1]
    half = own_ref.shape[0] // 2
    odd = lax.rem(lax.axis_index("kv"), 2)

    def total(part):
        add = back_ref[part].astype(jnp.float32) + other_ref[part].astype(jnp.float32)
        return (own_ref[part] + add).astype(jnp.bfloat16)

    if len(refs) > 1:
        refs[0][...] = total(slice(None)).reshape(refs[0].shape)
    grad_ref[...] = total(pl.ds(odd * half, half)).reshape(grad_ref.shape)


def prepare_kernel(
    piece, keys_ref, values_ref, inputs_ref, pair_ref, keep_ref, give_ref, rows, turned_rows, done
):
    width = keys_ref.shape[1]
    copies = [
        pltpu.make_async_copy(source, target, done.at[i])
        for i, (source, target) in enumerate(
            (
                (inputs_ref, rows),
                (keys_ref, pair_ref.at[:, pl.ds(0, width)]),
                (values_ref, pair_ref.at[:, pl.ds(width, width)]),
            )
        )
    ]
    for copy in copies:
        copy.start()
    for copy in copies:
        copy.wait()
    turned_rows[...] = rows[...].T
    corner = lax.rem(lax.axis_index("kv"), 4)
    for i in range(2):
        for out, owner in ((keep_ref, corner ^ (2 * i)), (give_ref, corner ^ (2 * i + 1))):
            for group in range(out.shape[1] // piece):
                out[i, pl.ds(group * piece, piece), :] = turned_rows[
                    pl.ds((4 * group + owner) * piece, piece), :
                ]


def join_kernel(keep_ref, got_ref, own_ref, across_ref):
    tokens = keep_ref.shape[2]
    odd = lax.rem(lax.axis_index("kv"), 2)
    for i, out in enumerate((own_ref, across_ref)):
        out[:, pl.ds(pl.multiple_of(odd * tokens, tokens), tokens)] = keep_ref[i]
        out[:, pl.ds(pl.multiple_of((1 - odd) * tokens, tokens), tokens)] = got_ref[i]


def partner(digit, step, radix):
    if radix & (radix - 1):
        return lax.rem(digit + step, radix)
    return digit ^ step


def product_kernel(shares, stride, radix, *refs):
    grads, factors = refs[:2], refs[2 : 2 + 2 * shares]
    outs = refs[2 + 2 * shares :]
    mine_ref, sends, result = outs[0], outs[1:radix], outs[radix]
    piece = result.shape[1]
    part = lax.axis_index("tp")
    per_share = factors[0].shape[0] // piece
    for step in range(shares):
        where = lax.rem(part + shares - step, shares)
        total = 0.0
        for i in range(2):
            total += jnp.dot(
                factors[2 * step + i][...], grads[i][...], preferred_element_type=jnp.float32
            )
        for i in range(per_share):
            result[where * per_share + i] = total[i * piece : (i + 1) * piece]
    digit = lax.rem(lax.axis_index("kv") // stride, radix)
    for i in range(mine_ref.shape[0]):
        mine_ref[i] = result[radix * i + digit]
        for s, send in enumerate(sends):
            send[i] = result[radix * i + partner(digit, s + 1, radix)].astype(jnp.bfloat16)


def spread_kernel(stride, radix, keep_ref, came_ref, *outs):
    mine_ref, sends = outs[0], outs[1:]
    digit = lax.rem(lax.axis_index("kv") // stride, radix)
    for i in range(mine_ref.shape[0]):
        at = radix * i + digit
        mine_ref[i] = keep_ref[at] + came_ref[at].astype(jnp.float32)
        for s, send in enumerate(sends):
            at = radix * i + partner(digit, s + 1, radix)
            send[i] = (keep_ref[at] + came_ref[at].astype(jnp.float32)).astype(jnp.bfloat16)


def spread(kept, came, stride, radix):
    shape = (kept.shape[0] // radix,) + kept.shape[1:]
    outs = [jax.ShapeDtypeStruct(shape, jnp.float32)]
    outs += [jax.ShapeDtypeStruct(shape, jnp.bfloat16)] * (radix - 1)
    return pl.pallas_call(
        functools.partial(spread_kernel, stride, radix),
        out_shape=outs,
        in_specs=vmem(2),
        out_specs=vmem(radix),
    )(kept, came)


def radices(count):
    found = []
    for radix in (4, 3, 2):
        while count % radix == 0:
            found.append(radix)
            count //= radix
    if count > 1:
        found.append(count)
    return found


def shards(queries, keys, values, log_sums, out_grad, chosen, inputs):
    tokens, width = keys.shape
    blocks = chosen.shape[0]
    block = tokens // blocks
    heads = queries.shape[1] // width
    slots = chosen.shape[2]
    count = lax.axis_size("kv")
    shares = lax.axis_size("tp")
    features = inputs.shape[1]
    piece = features * shares // count
    window = (REACH + 2) * blocks
    bf16, f32 = jnp.bfloat16, jnp.float32

    pair, keep, give = pl.pallas_call(
        functools.partial(prepare_kernel, piece),
        out_shape=[pltpu.VMEM((tokens, 2 * width), bf16)]
        + [pltpu.VMEM((2, features // 4, tokens), bf16)] * 2,
        in_specs=[pl.BlockSpec(memory_space=pltpu.HBM)] * 3,
        out_specs=vmem(3),
        scratch_shapes=[
            pltpu.VMEM((tokens, features), bf16),
            pltpu.VMEM((features, tokens), bf16),
            pltpu.SemaphoreType.DMA((3,)),
        ],
        compiler_params=PARAMS,
    )(*[pltpu.with_memory_space_constraint(v, pltpu.HBM) for v in (keys, values, inputs)])
    four = shifted(pair, 4)
    two = shifted(pair, 2)
    peer = swapped(pair, 1)
    peer_four = swapped(four, 1)
    peer_two = swapped(two, 1)

    got = swapped(give, 1)
    own_factor, across = pl.pallas_call(
        join_kernel,
        out_shape=[pltpu.VMEM((features // 4, 2 * tokens), bf16)] * 2,
        in_specs=vmem(2),
        out_specs=vmem(2),
        compiler_params=PARAMS,
    )(*near(keep, got))
    side_factor = swapped(across, 2)
    factors = [own_factor, side_factor]
    for step in range(1, shares):
        pairs = [(i, (i + step) % shares) for i in range(shares)]
        for i in range(2):
            factors.append(lax.ppermute(factors[i], "tp", pairs))

    query_grad, value_acc, value_low, key_acc, key_low = pl.pallas_call(
        functools.partial(attention_kernel, block, heads),
        out_shape=[
            pltpu.VMEM(queries.shape, bf16),
            pltpu.VMEM((window, block, width), f32),
            pltpu.VMEM((window, block, width), bf16),
            pltpu.VMEM((window, block, width), f32),
            pltpu.VMEM((window, block, width), bf16),
        ],
        in_specs=[pl.BlockSpec(memory_space=pltpu.SMEM)] + vmem(9),
        out_specs=vmem(5),
        scratch_shapes=[
            pltpu.VMEM((window, block, 2 * width), bf16),
            pltpu.VMEM(((slots + 1) * block, width), bf16),
            pltpu.VMEM(((slots + 1) * block, width), bf16),
        ],
        compiler_params=PARAMS,
    )(
        chosen,
        *near(queries, out_grad, log_sums, pair, two, four, peer, peer_two, peer_four),
    )

    def gathered(acc, low, both):
        came = swapped(low, 1)
        own, send = pl.pallas_call(
            chip_sum_kernel,
            out_shape=[
                pltpu.VMEM((2 * blocks, block, width), f32),
                pltpu.VMEM((2 * blocks, block, width), bf16),
            ],
            in_specs=vmem(2),
            out_specs=vmem(2),
            compiler_params=PARAMS,
        )(*near(acc, came))
        back = returned(send)
        other = swapped(back, 1)
        return pl.pallas_call(
            total_kernel,
            out_shape=[pltpu.VMEM((2 * tokens, width), bf16)] * both
            + [pltpu.VMEM((tokens, width), bf16)],
            in_specs=vmem(3),
            out_specs=vmem(both + 1),
            compiler_params=PARAMS,
        )(*near(own, back, other))

    value_both, value_grad = gathered(value_acc, value_low, 1)
    (key_grad,) = gathered(key_acc, key_low, 0)
    value_side = swapped(value_both, 2)

    pieces = count // 4
    stages = radices(pieces)
    kept, *sends = pl.pallas_call(
        functools.partial(product_kernel, shares, 4, stages[0]),
        out_shape=[pltpu.VMEM((pieces // stages[0], piece, width), f32)]
        + [pltpu.VMEM((pieces // stages[0], piece, width), bf16)] * (stages[0] - 1),
        in_specs=vmem(2 + 2 * shares),
        out_specs=vmem(stages[0]),
        scratch_shapes=[pltpu.VMEM((pieces, piece, width), f32)],
        compiler_params=PARAMS,
    )(*near(value_both, value_side, *factors))
    stride = 4
    for stage, radix in enumerate(stages):
        if stage:
            kept, *sends = spread(kept, came, stride, radix)
        came = 0.0
        for s, send in enumerate(sends):
            came = came + turned(send, stride, radix, s + 1).astype(f32)
        stride *= radix
    weight_grad = (kept + came)[0]
    return (query_grad, key_grad, value_grad, weight_grad)


def solution(mesh):
    in_specs = (
        P("kv", "tp"),
        P("kv", "tp"),
        P("kv", "tp"),
        P("tp", "kv"),
        P("kv", "tp"),
        P("kv", "tp", None),
        P("kv", "tp"),
    )
    out_specs = (P("kv", "tp"), P("kv", "tp"), P("kv", "tp"), P("kv", "tp"))

    return jax.shard_map(shards, mesh=mesh, in_specs=in_specs, out_specs=out_specs, check_vma=False)
```

```python
import functools

import jax
import jax.numpy as jnp
from jax import lax
from jax.experimental import pallas as pl
from jax.experimental.pallas import tpu as pltpu
from jax.sharding import PartitionSpec as P


REACH = 4
LOG2E = 1.4426950408889634


PARAMS = pltpu.CompilerParams(vmem_limit_bytes=24 << 20)


def vmem(count):
    return [pl.BlockSpec(memory_space=pltpu.VMEM)] * count


def near(*values):
    return [pltpu.with_memory_space_constraint(v, pltpu.VMEM) for v in values]


def far(*values):
    return [pltpu.with_memory_space_constraint(v, pltpu.HBM) for v in values]


def shifted(value, steps):
    count = lax.axis_size("kv")
    return lax.ppermute(value, "kv", [(i, (i + steps) % count) for i in range(count)])


def returned(value):
    count = lax.axis_size("kv")
    moves = [(i, (i - (4 if i % 2 else 2)) % count) for i in range(count)]
    return lax.ppermute(value, "kv", moves)


def swapped(value, bit):
    count = lax.axis_size("kv")
    return lax.ppermute(value, "kv", [(i, i ^ bit) for i in range(count)])


def turned(value, stride, radix, steps):
    count = lax.axis_size("kv")
    pairs = []
    for i in range(count):
        digit = i // stride % radix
        target = (digit + steps) % radix if radix & (radix - 1) else digit ^ steps
        pairs.append((i, i + (target - digit) * stride))
    return lax.ppermute(value, "kv", pairs)


def places_of(chosen_ref, b, blocks):
    device = lax.axis_index("kv")
    odd = lax.rem(device, 2)
    first = (device - odd - REACH) * blocks
    listed = [chosen_ref[b, 0, s] for s in range(chosen_ref.shape[2])]
    return [c - first for c in listed] + [(REACH + odd) * blocks + b], listed


def stacked(ref, b, block, width):
    heads = ref.shape[1] // width
    here = pl.ds(b * block, block)
    return jnp.concatenate([ref[here, pl.ds(a * width, width)] for a in range(heads)], 0)


def value_kernel(
    block,
    chosen_ref,
    queries_ref,
    out_grad_ref,
    sums_ref,
    own_ref,
    two_ref,
    four_ref,
    peer_ref,
    peer_two_ref,
    peer_four_ref,
    value_acc,
    value_low_ref,
    score_grads_ref,
    keys_ref,
    values,
    key_rows,
    value_rows,
):
    width = keys_ref.shape[2]
    heads = queries_ref.shape[1] // width
    blocks = queries_ref.shape[0] // block
    slots = chosen_ref.shape[2]
    scaling = width ** (-0.5)
    device = lax.axis_index("kv")
    odd = lax.rem(device, 2)

    def place(position, ref):
        for b in range(blocks):
            keys_ref[position * blocks + b] = ref[pl.ds(b * block, block), :width]
            values[position * blocks + b] = ref[pl.ds(b * block, block), width:]

    for back, (mine, theirs) in enumerate(
        ((own_ref, peer_ref), (two_ref, peer_two_ref), (four_ref, peer_four_ref))
    ):
        place(REACH - 2 * back + odd, mine)
        place(REACH - 2 * back + 1 - odd, theirs)

    value_acc[...] = jnp.zeros_like(value_acc)
    rows = heads * block
    key_pos = lax.broadcasted_iota(jnp.int32, (block, rows), 0)
    query_pos = lax.rem(lax.broadcasted_iota(jnp.int32, (block, rows), 1), block)
    causal = key_pos <= query_pos
    for b in range(blocks):
        here = pl.ds(b * block, block)
        places, listed = places_of(chosen_ref, b, blocks)
        offsets = [jnp.where(c < device * blocks + b, 0.0, 1e30) for c in listed] + [0.0]
        for s in range(slots + 1):
            key_rows[pl.ds(s * block, block), :] = keys_ref[places[s]]
            value_rows[pl.ds(s * block, block), :] = values[places[s]]
        q = stacked(queries_ref, b, block, width)
        g = stacked(out_grad_ref, b, block, width)
        sums = jnp.concatenate([sums_ref[pl.ds(a, 1), here] for a in range(heads)], 1) * LOG2E
        scores = lax.dot_general(
            key_rows[...], q, (((1,), (1,)), ((), ())), preferred_element_type=jnp.float32
        )
        grads = lax.dot_general(
            value_rows[...], g, (((1,), (1,)), ((), ())), preferred_element_type=jnp.float32
        )
        weights = []
        delta = jnp.zeros((1, rows), jnp.float32)
        for s in range(slots + 1):
            part = slice(s * block, (s + 1) * block)
            weight = jnp.exp2(scores[part] * (scaling * LOG2E) - (sums + offsets[s]))
            if s == slots:
                weight = jnp.where(causal, weight, 0.0)
            weights.append(weight)
            delta = delta + jnp.sum(weight * grads[part], 0, keepdims=True)
        for s in range(slots + 1):
            part = slice(s * block, (s + 1) * block)
            score_grad = weights[s] * (grads[part] - delta)
            score_grads_ref[b, pl.ds(s * block, block), :] = score_grad.astype(jnp.bfloat16)
        low = jnp.concatenate([w.astype(jnp.bfloat16) for w in weights], 0)
        value_part = jnp.dot(low, g, preferred_element_type=jnp.float32)
        for s in range(slots + 1):
            value_acc[places[s]] += value_part[s * block : (s + 1) * block]
    value_low_ref[...] = value_acc[...].astype(jnp.bfloat16)


def key_kernel(
    block,
    chosen_ref,
    queries_ref,
    score_grads_ref,
    keys_ref,
    query_grad_ref,
    key_acc,
    key_low_ref,
    key_rows,
):
    width = keys_ref.shape[2]
    heads = queries_ref.shape[1] // width
    blocks = queries_ref.shape[0] // block
    scaling = width ** (-0.5)
    key_acc[...] = jnp.zeros_like(key_acc)
    for b in range(blocks):
        places, _ = places_of(chosen_ref, b, blocks)
        for s, position in enumerate(places):
            key_rows[pl.ds(s * block, block), :] = keys_ref[position]
        score_grads = score_grads_ref[b]
        q = stacked(queries_ref, b, block, width)
        key_part = jnp.dot(score_grads, q, preferred_element_type=jnp.float32) * scaling
        query_part = lax.dot_general(
            score_grads, key_rows[...], (((0,), (0,)), ((), ())), preferred_element_type=jnp.float32
        )
        for a in range(heads):
            query_grad_ref[pl.ds(b * block, block), pl.ds(a * width, width)] = (
                query_part[a * block : (a + 1) * block] * scaling
            ).astype(jnp.bfloat16)
        for s, position in enumerate(places):
            key_acc[position] += key_part[s * block : (s + 1) * block]
    key_low_ref[...] = key_acc[...].astype(jnp.bfloat16)


def chip_sum_kernel(mine_ref, came_ref, own_ref, send_ref):
    half = own_ref.shape[0]
    odd = lax.rem(lax.axis_index("kv"), 2)
    last = mine_ref.shape[0] - half
    own_ref[...] = mine_ref[pl.ds(last, half)] + came_ref[pl.ds(last, half)].astype(jnp.float32)
    at = (1 - odd) * half
    total = mine_ref[pl.ds(at, half)] + came_ref[pl.ds(at, half)].astype(jnp.float32)
    send_ref[...] = total.astype(jnp.bfloat16)


def total_kernel(own_ref, back_ref, other_ref, *refs):
    grad_ref = refs[-1]
    half = own_ref.shape[0] // 2
    odd = lax.rem(lax.axis_index("kv"), 2)

    def total(part):
        add = back_ref[part].astype(jnp.float32) + other_ref[part].astype(jnp.float32)
        return (own_ref[part] + add).astype(jnp.bfloat16)

    if len(refs) > 1:
        refs[0][...] = total(slice(None)).reshape(refs[0].shape)
    grad_ref[...] = total(pl.ds(odd * half, half)).reshape(grad_ref.shape)


def pair_kernel(keys_ref, values_ref, pair_ref, done):
    width = keys_ref.shape[1]
    copies = [
        pltpu.make_async_copy(source, pair_ref.at[:, pl.ds(i * width, width)], done.at[i])
        for i, source in enumerate((keys_ref, values_ref))
    ]
    for copy in copies:
        copy.start()
    for copy in copies:
        copy.wait()


def transpose_kernel(piece, inputs_ref, keep_ref, give_ref, rows, turned_rows, done):
    copy = pltpu.make_async_copy(inputs_ref, rows, done)
    copy.start()
    copy.wait()
    turned_rows[...] = rows[...].T
    corner = lax.rem(lax.axis_index("kv"), 4)
    for i in range(2):
        for out, owner in ((keep_ref, corner ^ (2 * i)), (give_ref, corner ^ (2 * i + 1))):
            for group in range(out.shape[1] // piece):
                out[i, pl.ds(group * piece, piece), :] = turned_rows[
                    pl.ds((4 * group + owner) * piece, piece), :
                ]


def join_kernel(keep_ref, got_ref, own_ref, across_ref):
    tokens = keep_ref.shape[2]
    odd = lax.rem(lax.axis_index("kv"), 2)
    for i, out in enumerate((own_ref, across_ref)):
        out[:, pl.ds(pl.multiple_of(odd * tokens, tokens), tokens)] = keep_ref[i]
        out[:, pl.ds(pl.multiple_of((1 - odd) * tokens, tokens), tokens)] = got_ref[i]


def partner(digit, step, radix):
    if radix & (radix - 1):
        return lax.rem(digit + step, radix)
    return digit ^ step


def product_kernel(shares, stride, radix, *refs):
    grads, factors = refs[:2], refs[2 : 2 + 2 * shares]
    outs = refs[2 + 2 * shares :]
    mine_ref, sends, result = outs[0], outs[1:radix], outs[radix]
    piece = result.shape[1]
    part = lax.axis_index("tp")
    per_share = factors[0].shape[0] // piece
    for step in range(shares):
        where = lax.rem(part + shares - step, shares)
        total = 0.0
        for i in range(2):
            total += jnp.dot(
                factors[2 * step + i][...], grads[i][...], preferred_element_type=jnp.float32
            )
        for i in range(per_share):
            result[where * per_share + i] = total[i * piece : (i + 1) * piece]
    digit = lax.rem(lax.axis_index("kv") // stride, radix)
    for i in range(mine_ref.shape[0]):
        mine_ref[i] = result[radix * i + digit]
        for s, send in enumerate(sends):
            send[i] = result[radix * i + partner(digit, s + 1, radix)].astype(jnp.bfloat16)


def spread_kernel(stride, radix, keep_ref, came_ref, *outs):
    mine_ref, sends = outs[0], outs[1:]
    digit = lax.rem(lax.axis_index("kv") // stride, radix)
    for i in range(mine_ref.shape[0]):
        at = radix * i + digit
        mine_ref[i] = keep_ref[at] + came_ref[at].astype(jnp.float32)
        for s, send in enumerate(sends):
            at = radix * i + partner(digit, s + 1, radix)
            send[i] = (keep_ref[at] + came_ref[at].astype(jnp.float32)).astype(jnp.bfloat16)


def spread(kept, came, stride, radix):
    shape = (kept.shape[0] // radix,) + kept.shape[1:]
    outs = [jax.ShapeDtypeStruct(shape, jnp.float32)]
    outs += [jax.ShapeDtypeStruct(shape, jnp.bfloat16)] * (radix - 1)
    return pl.pallas_call(
        functools.partial(spread_kernel, stride, radix),
        out_shape=outs,
        in_specs=vmem(2),
        out_specs=vmem(radix),
    )(kept, came)


def radices(count):
    found = []
    for radix in (4, 3, 2):
        while count % radix == 0:
            found.append(radix)
            count //= radix
    if count > 1:
        found.append(count)
    return found


def shards(queries, keys, values, log_sums, out_grad, chosen, inputs):
    tokens, width = keys.shape
    blocks = chosen.shape[0]
    block = tokens // blocks
    heads = queries.shape[1] // width
    slots = chosen.shape[2]
    count = lax.axis_size("kv")
    shares = lax.axis_size("tp")
    features = inputs.shape[1]
    piece = features * shares // count
    window = (REACH + 2) * blocks
    bf16, f32 = jnp.bfloat16, jnp.float32

    pair = pl.pallas_call(
        pair_kernel,
        out_shape=pltpu.VMEM((tokens, 2 * width), bf16),
        in_specs=[pl.BlockSpec(memory_space=pltpu.HBM)] * 2,
        out_specs=pl.BlockSpec(memory_space=pltpu.VMEM),
        scratch_shapes=[pltpu.SemaphoreType.DMA((2,))],
        compiler_params=PARAMS,
    )(*far(keys, values))
    four = shifted(pair, 4)
    two = shifted(pair, 2)
    peer = swapped(pair, 1)
    peer_four = swapped(four, 1)
    peer_two = swapped(two, 1)

    keep, give = pl.pallas_call(
        functools.partial(transpose_kernel, piece),
        out_shape=[pltpu.VMEM((2, features // 4, tokens), bf16)] * 2,
        in_specs=[pl.BlockSpec(memory_space=pltpu.HBM)],
        out_specs=vmem(2),
        scratch_shapes=[
            pltpu.VMEM((tokens, features), bf16),
            pltpu.VMEM((features, tokens), bf16),
            pltpu.SemaphoreType.DMA,
        ],
        compiler_params=PARAMS,
    )(*far(inputs))
    got = swapped(give, 1)
    own_factor, across = pl.pallas_call(
        join_kernel,
        out_shape=[pltpu.VMEM((features // 4, 2 * tokens), bf16)] * 2,
        in_specs=vmem(2),
        out_specs=vmem(2),
        compiler_params=PARAMS,
    )(*near(keep, got))
    side_factor = swapped(across, 2)
    factors = [own_factor, side_factor]
    for step in range(1, shares):
        pairs = [(i, (i + step) % shares) for i in range(shares)]
        for i in range(2):
            factors.append(lax.ppermute(factors[i], "tp", pairs))

    queries, out_grad, log_sums = near(queries, out_grad, log_sums)
    value_acc, value_low, score_grads, window_keys = pl.pallas_call(
        functools.partial(value_kernel, block),
        out_shape=[
            pltpu.VMEM((window, block, width), f32),
            pltpu.VMEM((window, block, width), bf16),
            pltpu.VMEM((blocks, (slots + 1) * block, heads * block), bf16),
            pltpu.VMEM((window, block, width), bf16),
        ],
        in_specs=[pl.BlockSpec(memory_space=pltpu.SMEM)] + vmem(9),
        out_specs=vmem(4),
        scratch_shapes=[
            pltpu.VMEM((window, block, width), bf16),
            pltpu.VMEM(((slots + 1) * block, width), bf16),
            pltpu.VMEM(((slots + 1) * block, width), bf16),
        ],
        compiler_params=PARAMS,
    )(
        chosen,
        queries,
        out_grad,
        log_sums,
        *near(pair, two, four, peer, peer_two, peer_four),
    )
    query_grad, key_acc, key_low = pl.pallas_call(
        functools.partial(key_kernel, block),
        out_shape=[
            pltpu.VMEM(queries.shape, bf16),
            pltpu.VMEM((window, block, width), f32),
            pltpu.VMEM((window, block, width), bf16),
        ],
        in_specs=[pl.BlockSpec(memory_space=pltpu.SMEM)] + vmem(3),
        out_specs=vmem(3),
        scratch_shapes=[pltpu.VMEM(((slots + 1) * block, width), bf16)],
        compiler_params=PARAMS,
    )(chosen, queries, *near(score_grads, window_keys))

    def gathered(acc, low, both):
        came = swapped(low, 1)
        own, send = pl.pallas_call(
            chip_sum_kernel,
            out_shape=[
                pltpu.VMEM((2 * blocks, block, width), f32),
                pltpu.VMEM((2 * blocks, block, width), bf16),
            ],
            in_specs=vmem(2),
            out_specs=vmem(2),
            compiler_params=PARAMS,
        )(*near(acc, came))
        back = returned(send)
        other = swapped(back, 1)
        return pl.pallas_call(
            total_kernel,
            out_shape=[pltpu.VMEM((2 * tokens, width), bf16)] * both
            + [pltpu.VMEM((tokens, width), bf16)],
            in_specs=vmem(3),
            out_specs=vmem(both + 1),
            compiler_params=PARAMS,
        )(*near(own, back, other))

    value_both, value_grad = gathered(value_acc, value_low, 1)
    (key_grad,) = gathered(key_acc, key_low, 0)
    value_side = swapped(value_both, 2)

    pieces = count // 4
    stages = radices(pieces)
    kept, *sends = pl.pallas_call(
        functools.partial(product_kernel, shares, 4, stages[0]),
        out_shape=[pltpu.VMEM((pieces // stages[0], piece, width), f32)]
        + [pltpu.VMEM((pieces // stages[0], piece, width), bf16)] * (stages[0] - 1),
        in_specs=vmem(2 + 2 * shares),
        out_specs=vmem(stages[0]),
        scratch_shapes=[pltpu.VMEM((pieces, piece, width), f32)],
        compiler_params=PARAMS,
    )(*near(value_both, value_side, *factors))
    stride = 4
    for stage, radix in enumerate(stages):
        if stage:
            kept, *sends = spread(kept, came, stride, radix)
        came = 0.0
        for s, send in enumerate(sends):
            came = came + turned(send, stride, radix, s + 1).astype(f32)
        stride *= radix
    weight_grad = (kept + came)[0]
    return (query_grad, key_grad, value_grad, weight_grad)


def solution(mesh):
    in_specs = (
        P("kv", "tp"),
        P("kv", "tp"),
        P("kv", "tp"),
        P("tp", "kv"),
        P("kv", "tp"),
        P("kv", "tp", None),
        P("kv", "tp"),
    )
    out_specs = (P("kv", "tp"), P("kv", "tp"), P("kv", "tp"), P("kv", "tp"))

    return jax.shard_map(shards, mesh=mesh, in_specs=in_specs, out_specs=out_specs, check_vma=False)
```

```python
import functools

import jax
import jax.numpy as jnp
from jax import lax
from jax.experimental import pallas as pl
from jax.experimental.pallas import tpu as pltpu
from jax.sharding import PartitionSpec as P


REACH = 4
LOG2E = 1.4426950408889634


PARAMS = pltpu.CompilerParams(vmem_limit_bytes=24 << 20)


def vmem(count):
    return [pl.BlockSpec(memory_space=pltpu.VMEM)] * count


def near(*values):
    return [pltpu.with_memory_space_constraint(v, pltpu.VMEM) for v in values]


def far(*values):
    return [pltpu.with_memory_space_constraint(v, pltpu.HBM) for v in values]


def shifted(value, steps):
    count = lax.axis_size("kv")
    return lax.ppermute(value, "kv", [(i, (i + steps) % count) for i in range(count)])


def returned(value):
    count = lax.axis_size("kv")
    moves = [(i, (i - (4 if i % 2 else 2)) % count) for i in range(count)]
    return lax.ppermute(value, "kv", moves)


def swapped(value, bit):
    count = lax.axis_size("kv")
    return lax.ppermute(value, "kv", [(i, i ^ bit) for i in range(count)])


def turned(value, stride, radix, steps):
    count = lax.axis_size("kv")
    pairs = []
    for i in range(count):
        digit = i // stride % radix
        target = (digit + steps) % radix if radix & (radix - 1) else digit ^ steps
        pairs.append((i, i + (target - digit) * stride))
    return lax.ppermute(value, "kv", pairs)


def places_of(chosen_ref, b, blocks):
    device = lax.axis_index("kv")
    odd = lax.rem(device, 2)
    first = (device - odd - REACH) * blocks
    listed = [chosen_ref[b, 0, s] for s in range(chosen_ref.shape[2])]
    return [c - first for c in listed] + [(REACH + odd) * blocks + b], listed


def stacked(ref, b, block, width):
    heads = ref.shape[1] // width
    here = pl.ds(b * block, block)
    return jnp.concatenate([ref[here, pl.ds(a * width, width)] for a in range(heads)], 0)


def value_kernel(
    block,
    chosen_ref,
    queries_ref,
    out_grad_ref,
    sums_ref,
    own_ref,
    two_ref,
    four_ref,
    peer_ref,
    peer_two_ref,
    peer_four_ref,
    value_acc,
    value_low_ref,
    score_grads_ref,
    keys_ref,
    values,
    key_rows,
    value_rows,
):
    width = keys_ref.shape[2]
    heads = queries_ref.shape[1] // width
    blocks = queries_ref.shape[0] // block
    slots = chosen_ref.shape[2]
    scaling = width ** (-0.5)
    device = lax.axis_index("kv")
    odd = lax.rem(device, 2)

    def place(position, ref):
        for b in range(blocks):
            keys_ref[position * blocks + b] = ref[pl.ds(b * block, block), :width]
            values[position * blocks + b] = ref[pl.ds(b * block, block), width:]

    for back, (mine, theirs) in enumerate(
        ((own_ref, peer_ref), (two_ref, peer_two_ref), (four_ref, peer_four_ref))
    ):
        place(REACH - 2 * back + odd, mine)
        place(REACH - 2 * back + 1 - odd, theirs)

    value_acc[...] = jnp.zeros_like(value_acc)
    rows = heads * block
    key_pos = lax.broadcasted_iota(jnp.int32, (block, rows), 0)
    query_pos = lax.rem(lax.broadcasted_iota(jnp.int32, (block, rows), 1), block)
    causal = key_pos <= query_pos
    for b in range(blocks):
        here = pl.ds(b * block, block)
        places, listed = places_of(chosen_ref, b, blocks)
        offsets = [jnp.where(c < device * blocks + b, 0.0, 1e30) for c in listed] + [0.0]
        for s in range(slots + 1):
            key_rows[pl.ds(s * block, block), :] = keys_ref[places[s]]
            value_rows[pl.ds(s * block, block), :] = values[places[s]]
        q = stacked(queries_ref, b, block, width)
        g = stacked(out_grad_ref, b, block, width)
        sums = jnp.concatenate([sums_ref[pl.ds(a, 1), here] for a in range(heads)], 1) * LOG2E
        scores = lax.dot_general(
            key_rows[...], q, (((1,), (1,)), ((), ())), preferred_element_type=jnp.float32
        )
        grads = lax.dot_general(
            value_rows[...], g, (((1,), (1,)), ((), ())), preferred_element_type=jnp.float32
        )
        weights = []
        delta = jnp.zeros((1, rows), jnp.float32)
        for s in range(slots + 1):
            part = slice(s * block, (s + 1) * block)
            weight = jnp.exp2(scores[part] * (scaling * LOG2E) - (sums + offsets[s]))
            if s == slots:
                weight = jnp.where(causal, weight, 0.0)
            weights.append(weight)
            delta = delta + jnp.sum(weight * grads[part], 0, keepdims=True)
        for s in range(slots + 1):
            part = slice(s * block, (s + 1) * block)
            score_grad = weights[s] * (grads[part] - delta)
            score_grads_ref[b, pl.ds(s * block, block), :] = score_grad.astype(jnp.bfloat16)
        low = jnp.concatenate([w.astype(jnp.bfloat16) for w in weights], 0)
        value_part = jnp.dot(low, g, preferred_element_type=jnp.float32)
        for s in range(slots + 1):
            value_acc[places[s]] += value_part[s * block : (s + 1) * block]
    hand_over(value_acc, value_low_ref)


def key_kernel(
    block,
    chosen_ref,
    queries_ref,
    score_grads_ref,
    keys_ref,
    query_grad_ref,
    key_acc,
    key_low_ref,
    key_rows,
):
    width = keys_ref.shape[2]
    heads = queries_ref.shape[1] // width
    blocks = queries_ref.shape[0] // block
    scaling = width ** (-0.5)
    key_acc[...] = jnp.zeros_like(key_acc)
    for b in range(blocks):
        places, _ = places_of(chosen_ref, b, blocks)
        for s, position in enumerate(places):
            key_rows[pl.ds(s * block, block), :] = keys_ref[position]
        score_grads = score_grads_ref[b]
        q = stacked(queries_ref, b, block, width)
        key_part = jnp.dot(score_grads, q, preferred_element_type=jnp.float32) * scaling
        query_part = lax.dot_general(
            score_grads, key_rows[...], (((0,), (0,)), ((), ())), preferred_element_type=jnp.float32
        )
        for a in range(heads):
            query_grad_ref[pl.ds(b * block, block), pl.ds(a * width, width)] = (
                query_part[a * block : (a + 1) * block] * scaling
            ).astype(jnp.bfloat16)
        for s, position in enumerate(places):
            key_acc[position] += key_part[s * block : (s + 1) * block]
    hand_over(key_acc, key_low_ref)


def hand_over(acc_ref, low_ref):
    half = low_ref.shape[0] // 2
    odd = lax.rem(lax.axis_index("kv"), 2)
    low_ref[:half] = acc_ref[pl.ds(odd * half, half)].astype(jnp.bfloat16)
    low_ref[half:] = acc_ref[2 * half :].astype(jnp.bfloat16)


def chip_sum_kernel(mine_ref, came_ref, own_ref, send_ref):
    half = own_ref.shape[0]
    odd = lax.rem(lax.axis_index("kv"), 2)
    own_ref[...] = mine_ref[2 * half :] + came_ref[half:].astype(jnp.float32)
    total = mine_ref[pl.ds((1 - odd) * half, half)] + came_ref[:half].astype(jnp.float32)
    send_ref[...] = total.astype(jnp.bfloat16)


def total_kernel(own_ref, back_ref, other_ref, *refs):
    grad_ref = refs[-1]
    half = own_ref.shape[0] // 2
    odd = lax.rem(lax.axis_index("kv"), 2)

    def total(part):
        add = back_ref[part].astype(jnp.float32) + other_ref[part].astype(jnp.float32)
        return (own_ref[part] + add).astype(jnp.bfloat16)

    if len(refs) > 1:
        refs[0][...] = total(slice(None)).reshape(refs[0].shape)
    grad_ref[...] = total(pl.ds(odd * half, half)).reshape(grad_ref.shape)


def pair_kernel(keys_ref, values_ref, inputs_ref, pair_ref, rows_ref, done):
    width = keys_ref.shape[1]
    copies = [
        pltpu.make_async_copy(source, target, done.at[i])
        for i, (source, target) in enumerate(
            (
                (keys_ref, pair_ref.at[:, pl.ds(0, width)]),
                (values_ref, pair_ref.at[:, pl.ds(width, width)]),
                (inputs_ref, rows_ref),
            )
        )
    ]
    for copy in copies:
        copy.start()
    for copy in copies:
        copy.wait()


def transpose_kernel(piece, rows_ref, keep_ref, give_ref, turned_rows):
    turned_rows[...] = rows_ref[...].T
    corner = lax.rem(lax.axis_index("kv"), 4)
    for i in range(2):
        for out, owner in ((keep_ref, corner ^ (2 * i)), (give_ref, corner ^ (2 * i + 1))):
            for group in range(out.shape[1] // piece):
                out[i, pl.ds(group * piece, piece), :] = turned_rows[
                    pl.ds((4 * group + owner) * piece, piece), :
                ]


def join_kernel(keep_ref, got_ref, own_ref, across_ref):
    tokens = keep_ref.shape[2]
    odd = lax.rem(lax.axis_index("kv"), 2)
    for i, out in enumerate((own_ref, across_ref)):
        out[:, pl.ds(pl.multiple_of(odd * tokens, tokens), tokens)] = keep_ref[i]
        out[:, pl.ds(pl.multiple_of((1 - odd) * tokens, tokens), tokens)] = got_ref[i]


def partner(digit, step, radix):
    if radix & (radix - 1):
        return lax.rem(digit + step, radix)
    return digit ^ step


def product_kernel(shares, stride, radix, *refs):
    grads, factors = refs[:2], refs[2 : 2 + 2 * shares]
    outs = refs[2 + 2 * shares :]
    mine_ref, sends, result = outs[0], outs[1:radix], outs[radix]
    piece = result.shape[1]
    part = lax.axis_index("tp")
    per_share = factors[0].shape[0] // piece
    for step in range(shares):
        where = lax.rem(part + shares - step, shares)
        total = 0.0
        for i in range(2):
            total += jnp.dot(
                factors[2 * step + i][...], grads[i][...], preferred_element_type=jnp.float32
            )
        for i in range(per_share):
            result[where * per_share + i] = total[i * piece : (i + 1) * piece]
    digit = lax.rem(lax.axis_index("kv") // stride, radix)
    for i in range(mine_ref.shape[0]):
        mine_ref[i] = result[radix * i + digit]
        for s, send in enumerate(sends):
            send[i] = result[radix * i + partner(digit, s + 1, radix)].astype(jnp.bfloat16)


def spread_kernel(stride, radix, keep_ref, came_ref, *outs):
    mine_ref, sends = outs[0], outs[1:]
    digit = lax.rem(lax.axis_index("kv") // stride, radix)
    for i in range(mine_ref.shape[0]):
        at = radix * i + digit
        mine_ref[i] = keep_ref[at] + came_ref[at].astype(jnp.float32)
        for s, send in enumerate(sends):
            at = radix * i + partner(digit, s + 1, radix)
            send[i] = (keep_ref[at] + came_ref[at].astype(jnp.float32)).astype(jnp.bfloat16)


def spread(kept, came, stride, radix):
    shape = (kept.shape[0] // radix,) + kept.shape[1:]
    outs = [jax.ShapeDtypeStruct(shape, jnp.float32)]
    outs += [jax.ShapeDtypeStruct(shape, jnp.bfloat16)] * (radix - 1)
    return pl.pallas_call(
        functools.partial(spread_kernel, stride, radix),
        out_shape=outs,
        in_specs=vmem(2),
        out_specs=vmem(radix),
    )(kept, came)


def radices(count):
    found = []
    for radix in (4, 3, 2):
        while count % radix == 0:
            found.append(radix)
            count //= radix
    if count > 1:
        found.append(count)
    return found


def shards(queries, keys, values, log_sums, out_grad, chosen, inputs):
    tokens, width = keys.shape
    blocks = chosen.shape[0]
    block = tokens // blocks
    heads = queries.shape[1] // width
    slots = chosen.shape[2]
    count = lax.axis_size("kv")
    shares = lax.axis_size("tp")
    features = inputs.shape[1]
    piece = features * shares // count
    window = (REACH + 2) * blocks
    bf16, f32 = jnp.bfloat16, jnp.float32

    pair, rows = pl.pallas_call(
        pair_kernel,
        out_shape=[pltpu.VMEM((tokens, 2 * width), bf16), pltpu.VMEM(inputs.shape, bf16)],
        in_specs=[pl.BlockSpec(memory_space=pltpu.HBM)] * 3,
        out_specs=vmem(2),
        scratch_shapes=[pltpu.SemaphoreType.DMA((3,))],
        compiler_params=PARAMS,
    )(*far(keys, values, inputs))
    four = shifted(pair, 4)
    two = shifted(pair, 2)
    peer = swapped(pair, 1)
    peer_four = swapped(four, 1)
    peer_two = swapped(two, 1)

    keep, give = pl.pallas_call(
        functools.partial(transpose_kernel, piece),
        out_shape=[pltpu.VMEM((2, features // 4, tokens), bf16)] * 2,
        in_specs=vmem(1),
        out_specs=vmem(2),
        scratch_shapes=[pltpu.VMEM((features, tokens), bf16)],
        compiler_params=PARAMS,
    )(*near(rows))
    got = swapped(give, 1)
    own_factor, across = pl.pallas_call(
        join_kernel,
        out_shape=[pltpu.VMEM((features // 4, 2 * tokens), bf16)] * 2,
        in_specs=vmem(2),
        out_specs=vmem(2),
        compiler_params=PARAMS,
    )(*near(keep, got))
    side_factor = swapped(across, 2)
    factors = [own_factor, side_factor]
    for step in range(1, shares):
        pairs = [(i, (i + step) % shares) for i in range(shares)]
        for i in range(2):
            factors.append(lax.ppermute(factors[i], "tp", pairs))

    queries, out_grad, log_sums = near(queries, out_grad, log_sums)
    value_acc, value_low, score_grads, window_keys = pl.pallas_call(
        functools.partial(value_kernel, block),
        out_shape=[
            pltpu.VMEM((window, block, width), f32),
            pltpu.VMEM((4 * blocks, block, width), bf16),
            pltpu.VMEM((blocks, (slots + 1) * block, heads * block), bf16),
            pltpu.VMEM((window, block, width), bf16),
        ],
        in_specs=[pl.BlockSpec(memory_space=pltpu.SMEM)] + vmem(9),
        out_specs=vmem(4),
        scratch_shapes=[
            pltpu.VMEM((window, block, width), bf16),
            pltpu.VMEM(((slots + 1) * block, width), bf16),
            pltpu.VMEM(((slots + 1) * block, width), bf16),
        ],
        compiler_params=PARAMS,
    )(
        chosen,
        queries,
        out_grad,
        log_sums,
        *near(pair, two, four, peer, peer_two, peer_four),
    )
    query_grad, key_acc, key_low = pl.pallas_call(
        functools.partial(key_kernel, block),
        out_shape=[
            pltpu.VMEM(queries.shape, bf16),
            pltpu.VMEM((window, block, width), f32),
            pltpu.VMEM((4 * blocks, block, width), bf16),
        ],
        in_specs=[pl.BlockSpec(memory_space=pltpu.SMEM)] + vmem(3),
        out_specs=vmem(3),
        scratch_shapes=[pltpu.VMEM(((slots + 1) * block, width), bf16)],
        compiler_params=PARAMS,
    )(chosen, queries, *near(score_grads, window_keys))

    def gathered(acc, low, both):
        came = swapped(low, 1)
        own, send = pl.pallas_call(
            chip_sum_kernel,
            out_shape=[
                pltpu.VMEM((2 * blocks, block, width), f32),
                pltpu.VMEM((2 * blocks, block, width), bf16),
            ],
            in_specs=vmem(2),
            out_specs=vmem(2),
            compiler_params=PARAMS,
        )(*near(acc, came))
        back = returned(send)
        other = swapped(back, 1)
        return pl.pallas_call(
            total_kernel,
            out_shape=[pltpu.VMEM((2 * tokens, width), bf16)] * both
            + [pltpu.VMEM((tokens, width), bf16)],
            in_specs=vmem(3),
            out_specs=vmem(both + 1),
            compiler_params=PARAMS,
        )(*near(own, back, other))

    value_both, value_grad = gathered(value_acc, value_low, 1)
    (key_grad,) = gathered(key_acc, key_low, 0)
    value_side = swapped(value_both, 2)

    pieces = count // 4
    stages = radices(pieces)
    kept, *sends = pl.pallas_call(
        functools.partial(product_kernel, shares, 4, stages[0]),
        out_shape=[pltpu.VMEM((pieces // stages[0], piece, width), f32)]
        + [pltpu.VMEM((pieces // stages[0], piece, width), bf16)] * (stages[0] - 1),
        in_specs=vmem(2 + 2 * shares),
        out_specs=vmem(stages[0]),
        scratch_shapes=[pltpu.VMEM((pieces, piece, width), f32)],
        compiler_params=PARAMS,
    )(*near(value_both, value_side, *factors))
    stride = 4
    for stage, radix in enumerate(stages):
        if stage:
            kept, *sends = spread(kept, came, stride, radix)
        came = 0.0
        for s, send in enumerate(sends):
            came = came + turned(send, stride, radix, s + 1).astype(f32)
        stride *= radix
    weight_grad = (kept + came)[0]
    return (query_grad, key_grad, value_grad, weight_grad)


def solution(mesh):
    in_specs = (
        P("kv", "tp"),
        P("kv", "tp"),
        P("kv", "tp"),
        P("tp", "kv"),
        P("kv", "tp"),
        P("kv", "tp", None),
        P("kv", "tp"),
    )
    out_specs = (P("kv", "tp"), P("kv", "tp"), P("kv", "tp"), P("kv", "tp"))

    return jax.shard_map(shards, mesh=mesh, in_specs=in_specs, out_specs=out_specs, check_vma=False)
```

```python
import functools

import jax
import jax.numpy as jnp
from jax import lax
from jax.experimental import pallas as pl
from jax.experimental.pallas import tpu as pltpu
from jax.sharding import PartitionSpec as P


REACH = 4
LOG2E = 1.4426950408889634


PARAMS = pltpu.CompilerParams(vmem_limit_bytes=24 << 20)


def vmem(count):
    return [pl.BlockSpec(memory_space=pltpu.VMEM)] * count


def near(*values):
    return [pltpu.with_memory_space_constraint(v, pltpu.VMEM) for v in values]


def far(*values):
    return [pltpu.with_memory_space_constraint(v, pltpu.HBM) for v in values]


def shifted(value, steps):
    count = lax.axis_size("kv")
    return lax.ppermute(value, "kv", [(i, (i + steps) % count) for i in range(count)])


def returned(value):
    count = lax.axis_size("kv")
    moves = [(i, (i - (4 if i % 2 else 2)) % count) for i in range(count)]
    return lax.ppermute(value, "kv", moves)


def swapped(value, bit):
    count = lax.axis_size("kv")
    return lax.ppermute(value, "kv", [(i, i ^ bit) for i in range(count)])


def turned(value, stride, radix, steps):
    count = lax.axis_size("kv")
    pairs = []
    for i in range(count):
        digit = i // stride % radix
        target = (digit + steps) % radix if radix & (radix - 1) else digit ^ steps
        pairs.append((i, i + (target - digit) * stride))
    return lax.ppermute(value, "kv", pairs)


def places_of(chosen_ref, b, blocks):
    device = lax.axis_index("kv")
    odd = lax.rem(device, 2)
    first = (device - odd - REACH) * blocks
    listed = [chosen_ref[b, 0, s] for s in range(chosen_ref.shape[2])]
    return [c - first for c in listed] + [(REACH + odd) * blocks + b], listed


def stacked(ref, b, block, width):
    heads = ref.shape[1] // width
    here = pl.ds(b * block, block)
    return jnp.concatenate([ref[here, pl.ds(a * width, width)] for a in range(heads)], 0)


def value_kernel(
    block,
    chosen_ref,
    queries_ref,
    out_grad_ref,
    sums_ref,
    own_ref,
    two_ref,
    four_ref,
    peer_ref,
    peer_two_ref,
    peer_four_ref,
    value_acc,
    value_low_ref,
    score_grads_ref,
    keys_ref,
    values,
    key_rows,
    value_rows,
):
    width = keys_ref.shape[2]
    heads = queries_ref.shape[1] // width
    blocks = queries_ref.shape[0] // block
    slots = chosen_ref.shape[2]
    scaling = width ** (-0.5)
    device = lax.axis_index("kv")
    odd = lax.rem(device, 2)

    def place(position, ref):
        for b in range(blocks):
            keys_ref[position * blocks + b] = ref[pl.ds(b * block, block), :width]
            values[position * blocks + b] = ref[pl.ds(b * block, block), width:]

    for back, (mine, theirs) in enumerate(
        ((own_ref, peer_ref), (two_ref, peer_two_ref), (four_ref, peer_four_ref))
    ):
        place(REACH - 2 * back + odd, mine)
        place(REACH - 2 * back + 1 - odd, theirs)

    value_acc[...] = jnp.zeros_like(value_acc)
    rows = heads * block
    key_pos = lax.broadcasted_iota(jnp.int32, (block, rows), 0)
    query_pos = lax.rem(lax.broadcasted_iota(jnp.int32, (block, rows), 1), block)
    causal = key_pos <= query_pos
    for b in range(blocks):
        here = pl.ds(b * block, block)
        places, listed = places_of(chosen_ref, b, blocks)
        offsets = [jnp.where(c < device * blocks + b, 0.0, 1e30) for c in listed] + [0.0]
        for s in range(slots + 1):
            key_rows[pl.ds(s * block, block), :] = keys_ref[places[s]]
            value_rows[pl.ds(s * block, block), :] = values[places[s]]
        q = stacked(queries_ref, b, block, width)
        g = stacked(out_grad_ref, b, block, width)
        sums = jnp.concatenate([sums_ref[pl.ds(a, 1), here] for a in range(heads)], 1) * LOG2E
        scores = lax.dot_general(
            key_rows[...], q, (((1,), (1,)), ((), ())), preferred_element_type=jnp.float32
        )
        grads = lax.dot_general(
            value_rows[...], g, (((1,), (1,)), ((), ())), preferred_element_type=jnp.float32
        )
        weights = []
        delta = jnp.zeros((1, rows), jnp.float32)
        for s in range(slots + 1):
            part = slice(s * block, (s + 1) * block)
            weight = jnp.exp2(scores[part] * (scaling * LOG2E) - (sums + offsets[s]))
            if s == slots:
                weight = jnp.where(causal, weight, 0.0)
            weights.append(weight)
            delta = delta + jnp.sum(weight * grads[part], 0, keepdims=True)
        for s in range(slots + 1):
            part = slice(s * block, (s + 1) * block)
            score_grad = weights[s] * (grads[part] - delta)
            score_grads_ref[b, pl.ds(s * block, block), :] = score_grad.astype(jnp.bfloat16)
        low = jnp.concatenate([w.astype(jnp.bfloat16) for w in weights], 0)
        value_part = jnp.dot(low, g, preferred_element_type=jnp.float32)
        for s in range(slots + 1):
            value_acc[places[s]] += value_part[s * block : (s + 1) * block]
    hand_over(value_acc, value_low_ref)


def key_kernel(
    block,
    chosen_ref,
    queries_ref,
    score_grads_ref,
    keys_ref,
    query_grad_ref,
    key_acc,
    key_low_ref,
    key_rows,
):
    width = keys_ref.shape[2]
    heads = queries_ref.shape[1] // width
    blocks = queries_ref.shape[0] // block
    scaling = width ** (-0.5)
    key_acc[...] = jnp.zeros_like(key_acc)
    for b in range(blocks):
        places, _ = places_of(chosen_ref, b, blocks)
        for s, position in enumerate(places):
            key_rows[pl.ds(s * block, block), :] = keys_ref[position]
        score_grads = score_grads_ref[b]
        q = stacked(queries_ref, b, block, width)
        key_part = jnp.dot(score_grads, q, preferred_element_type=jnp.float32) * scaling
        query_part = lax.dot_general(
            score_grads, key_rows[...], (((0,), (0,)), ((), ())), preferred_element_type=jnp.float32
        )
        for a in range(heads):
            query_grad_ref[pl.ds(b * block, block), pl.ds(a * width, width)] = (
                query_part[a * block : (a + 1) * block] * scaling
            ).astype(jnp.bfloat16)
        for s, position in enumerate(places):
            key_acc[position] += key_part[s * block : (s + 1) * block]
    hand_over(key_acc, key_low_ref)


def hand_over(acc_ref, low_ref):
    half = low_ref.shape[0] // 2
    odd = lax.rem(lax.axis_index("kv"), 2)
    low_ref[:half] = acc_ref[pl.ds(odd * half, half)].astype(jnp.bfloat16)
    low_ref[half:] = acc_ref[2 * half :].astype(jnp.bfloat16)


def chip_sum_kernel(mine_ref, came_ref, own_ref, send_ref):
    half = own_ref.shape[0]
    odd = lax.rem(lax.axis_index("kv"), 2)
    own_ref[...] = mine_ref[2 * half :] + came_ref[half:].astype(jnp.float32)
    total = mine_ref[pl.ds((1 - odd) * half, half)] + came_ref[:half].astype(jnp.float32)
    send_ref[...] = total.astype(jnp.bfloat16)


def total_kernel(own_ref, back_ref, other_ref, *refs):
    grad_ref = refs[-1]
    half = own_ref.shape[0] // 2
    odd = lax.rem(lax.axis_index("kv"), 2)

    def total(part):
        add = back_ref[part].astype(jnp.float32) + other_ref[part].astype(jnp.float32)
        return (own_ref[part] + add).astype(jnp.bfloat16)

    if len(refs) > 1:
        refs[0][...] = total(slice(None)).reshape(refs[0].shape)
    grad_ref[...] = total(pl.ds(odd * half, half)).reshape(grad_ref.shape)


def pair_kernel(keys_ref, values_ref, inputs_ref, pair_ref, rows_ref, done):
    width = keys_ref.shape[1]
    copies = [
        pltpu.make_async_copy(source, target, done.at[i])
        for i, (source, target) in enumerate(
            (
                (keys_ref, pair_ref.at[:, pl.ds(0, width)]),
                (values_ref, pair_ref.at[:, pl.ds(width, width)]),
                (inputs_ref, rows_ref),
            )
        )
    ]
    for copy in copies:
        copy.start()
    for copy in copies:
        copy.wait()


def transpose_kernel(piece, rows_ref, keep_ref, give_ref, turned_rows):
    turned_rows[...] = rows_ref[...].T
    corner = lax.rem(lax.axis_index("kv"), 4)
    for i in range(2):
        for out, owner in ((keep_ref, corner ^ (2 * i)), (give_ref, corner ^ (2 * i + 1))):
            for group in range(out.shape[1] // piece):
                out[i, pl.ds(group * piece, piece), :] = turned_rows[
                    pl.ds((4 * group + owner) * piece, piece), :
                ]


def join_kernel(keep_ref, got_ref, own_ref, across_ref):
    tokens = keep_ref.shape[2]
    odd = lax.rem(lax.axis_index("kv"), 2)
    for i, out in enumerate((own_ref, across_ref)):
        out[:, pl.ds(pl.multiple_of(odd * tokens, tokens), tokens)] = keep_ref[i]
        out[:, pl.ds(pl.multiple_of((1 - odd) * tokens, tokens), tokens)] = got_ref[i]


def partner(digit, step, radix):
    if radix & (radix - 1):
        return lax.rem(digit + step, radix)
    return digit ^ step


def product_kernel(shares, grads_ref, *refs):
    factors, out = refs[:shares], refs[shares]
    piece = out.shape[1]
    per_share = factors[0].shape[0] // piece
    part = lax.axis_index("tp")
    for step in range(shares):
        where = lax.rem(part + shares - step, shares)
        total = jnp.dot(factors[step][...], grads_ref[...], preferred_element_type=jnp.float32)
        for i in range(per_share):
            out[where * per_share + i] = total[i * piece : (i + 1) * piece].astype(out.dtype)


def spread_kernel(stride, radix, keep_ref, came_ref, *outs):
    mine_ref, sends = outs[0], outs[1:]
    digit = lax.rem(lax.axis_index("kv") // stride, radix)
    for i in range(mine_ref.shape[0]):
        at = radix * i + digit
        mine_ref[i] = keep_ref[at] + came_ref[at].astype(jnp.float32)
        for s, send in enumerate(sends):
            at = radix * i + partner(digit, s + 1, radix)
            send[i] = (keep_ref[at] + came_ref[at].astype(jnp.float32)).astype(jnp.bfloat16)


def spread(kept, came, stride, radix):
    shape = (kept.shape[0] // radix,) + kept.shape[1:]
    return pl.pallas_call(
        functools.partial(spread_kernel, stride, radix),
        out_shape=[pltpu.VMEM(shape, jnp.float32)] + [pltpu.VMEM(shape, jnp.bfloat16)] * (radix - 1),
        in_specs=vmem(2),
        out_specs=vmem(radix),
        compiler_params=PARAMS,
    )(*near(kept, came))


def radices(count):
    found = []
    for radix in (4, 3, 2):
        while count % radix == 0:
            found.append(radix)
            count //= radix
    if count > 1:
        found.append(count)
    return found


def shards(queries, keys, values, log_sums, out_grad, chosen, inputs):
    tokens, width = keys.shape
    blocks = chosen.shape[0]
    block = tokens // blocks
    heads = queries.shape[1] // width
    slots = chosen.shape[2]
    count = lax.axis_size("kv")
    shares = lax.axis_size("tp")
    features = inputs.shape[1]
    piece = features * shares // count
    window = (REACH + 2) * blocks
    bf16, f32 = jnp.bfloat16, jnp.float32

    pair, rows = pl.pallas_call(
        pair_kernel,
        out_shape=[pltpu.VMEM((tokens, 2 * width), bf16), pltpu.VMEM(inputs.shape, bf16)],
        in_specs=[pl.BlockSpec(memory_space=pltpu.HBM)] * 3,
        out_specs=vmem(2),
        scratch_shapes=[pltpu.SemaphoreType.DMA((3,))],
        compiler_params=PARAMS,
    )(*far(keys, values, inputs))
    four = shifted(pair, 4)
    two = shifted(pair, 2)
    peer = swapped(pair, 1)
    peer_four = swapped(four, 1)
    peer_two = swapped(two, 1)

    keep, give = pl.pallas_call(
        functools.partial(transpose_kernel, piece),
        out_shape=[pltpu.VMEM((2, features // 4, tokens), bf16)] * 2,
        in_specs=vmem(1),
        out_specs=vmem(2),
        scratch_shapes=[pltpu.VMEM((features, tokens), bf16)],
        compiler_params=PARAMS,
    )(*near(rows))
    got = swapped(give, 1)
    own_factor, across = pl.pallas_call(
        join_kernel,
        out_shape=[pltpu.VMEM((features // 4, 2 * tokens), bf16)] * 2,
        in_specs=vmem(2),
        out_specs=vmem(2),
        compiler_params=PARAMS,
    )(*near(keep, got))
    own_factors, across_factors = [own_factor], [across]
    for step in range(1, shares):
        pairs = [(i, (i + step) % shares) for i in range(shares)]
        across_factors.append(lax.ppermute(across, "tp", pairs))
        own_factors.append(lax.ppermute(own_factor, "tp", pairs))

    queries, out_grad, log_sums = near(queries, out_grad, log_sums)
    value_acc, value_low, score_grads, window_keys = pl.pallas_call(
        functools.partial(value_kernel, block),
        out_shape=[
            pltpu.VMEM((window, block, width), f32),
            pltpu.VMEM((4 * blocks, block, width), bf16),
            pltpu.VMEM((blocks, (slots + 1) * block, heads * block), bf16),
            pltpu.VMEM((window, block, width), bf16),
        ],
        in_specs=[pl.BlockSpec(memory_space=pltpu.SMEM)] + vmem(9),
        out_specs=vmem(4),
        scratch_shapes=[
            pltpu.VMEM((window, block, width), bf16),
            pltpu.VMEM(((slots + 1) * block, width), bf16),
            pltpu.VMEM(((slots + 1) * block, width), bf16),
        ],
        compiler_params=PARAMS,
    )(
        chosen,
        queries,
        out_grad,
        log_sums,
        *near(pair, two, four, peer, peer_two, peer_four),
    )
    query_grad, key_acc, key_low = pl.pallas_call(
        functools.partial(key_kernel, block),
        out_shape=[
            pltpu.VMEM(queries.shape, bf16),
            pltpu.VMEM((window, block, width), f32),
            pltpu.VMEM((4 * blocks, block, width), bf16),
        ],
        in_specs=[pl.BlockSpec(memory_space=pltpu.SMEM)] + vmem(3),
        out_specs=vmem(3),
        scratch_shapes=[pltpu.VMEM(((slots + 1) * block, width), bf16)],
        compiler_params=PARAMS,
    )(chosen, queries, *near(score_grads, window_keys))

    def gathered(acc, low, both):
        came = swapped(low, 1)
        own, send = pl.pallas_call(
            chip_sum_kernel,
            out_shape=[
                pltpu.VMEM((2 * blocks, block, width), f32),
                pltpu.VMEM((2 * blocks, block, width), bf16),
            ],
            in_specs=vmem(2),
            out_specs=vmem(2),
            compiler_params=PARAMS,
        )(*near(acc, came))
        back = returned(send)
        other = swapped(back, 1)
        return pl.pallas_call(
            total_kernel,
            out_shape=[pltpu.VMEM((2 * tokens, width), bf16)] * both
            + [pltpu.VMEM((tokens, width), bf16)],
            in_specs=vmem(3),
            out_specs=vmem(both + 1),
            compiler_params=PARAMS,
        )(*near(own, back, other))

    value_both, value_grad = gathered(value_acc, value_low, 1)
    (key_grad,) = gathered(key_acc, key_low, 0)

    pieces = count // 4

    def product(factors, dtype):
        return pl.pallas_call(
            functools.partial(product_kernel, shares),
            out_shape=pltpu.VMEM((pieces, piece, width), dtype),
            in_specs=vmem(1 + shares),
            out_specs=pl.BlockSpec(memory_space=pltpu.VMEM),
            compiler_params=PARAMS,
        )(*near(value_both, *factors))

    sent = product(across_factors, bf16)
    came = swapped(sent, 2)
    kept = product(own_factors, f32)
    stride = 4
    for radix in radices(pieces):
        kept, *sends = spread(kept, came, stride, radix)
        came = 0.0
        for s, send in enumerate(sends):
            came = came + turned(send, stride, radix, s + 1).astype(f32)
        stride *= radix
    weight_grad = (kept + came)[0]
    return (query_grad, key_grad, value_grad, weight_grad)


def solution(mesh):
    in_specs = (
        P("kv", "tp"),
        P("kv", "tp"),
        P("kv", "tp"),
        P("tp", "kv"),
        P("kv", "tp"),
        P("kv", "tp", None),
        P("kv", "tp"),
    )
    out_specs = (P("kv", "tp"), P("kv", "tp"), P("kv", "tp"), P("kv", "tp"))

    return jax.shard_map(shards, mesh=mesh, in_specs=in_specs, out_specs=out_specs, check_vma=False)
```

```python
import functools

import jax
import jax.numpy as jnp
from jax import lax
from jax.experimental import pallas as pl
from jax.experimental.pallas import tpu as pltpu
from jax.sharding import PartitionSpec as P


REACH = 4
LOG2E = 1.4426950408889634


PARAMS = pltpu.CompilerParams(vmem_limit_bytes=24 << 20)


def vmem(count):
    return [pl.BlockSpec(memory_space=pltpu.VMEM)] * count


def near(*values):
    return [pltpu.with_memory_space_constraint(v, pltpu.VMEM) for v in values]


def far(*values):
    return [pltpu.with_memory_space_constraint(v, pltpu.HBM) for v in values]


def shifted(value, steps):
    count = lax.axis_size("kv")
    return lax.ppermute(value, "kv", [(i, (i + steps) % count) for i in range(count)])


def exchanged(value, phase):
    count = lax.axis_size("kv")
    pairs = []
    for i in range(count):
        other = i + (4 if (i // 4 + phase) % 2 == 0 else -4)
        pairs.append((i, other if 0 <= other < count else i))
    return lax.ppermute(value, "kv", pairs)


def returned(value):
    count = lax.axis_size("kv")
    moves = [(i, (i - (4 if i % 2 else 2)) % count) for i in range(count)]
    return lax.ppermute(value, "kv", moves)


def swapped(value, bit):
    count = lax.axis_size("kv")
    return lax.ppermute(value, "kv", [(i, i ^ bit) for i in range(count)])


def turned(value, stride, radix, steps):
    count = lax.axis_size("kv")
    pairs = []
    for i in range(count):
        digit = i // stride % radix
        target = (digit + steps) % radix if radix & (radix - 1) else digit ^ steps
        pairs.append((i, i + (target - digit) * stride))
    return lax.ppermute(value, "kv", pairs)


def places_of(chosen_ref, b, blocks):
    device = lax.axis_index("kv")
    odd = lax.rem(device, 2)
    first = (device - odd - REACH) * blocks
    listed = [chosen_ref[b, 0, s] for s in range(chosen_ref.shape[2])]
    return [c - first for c in listed] + [(REACH + odd) * blocks + b], listed


def stacked(ref, b, block, width):
    heads = ref.shape[1] // width
    here = pl.ds(b * block, block)
    return jnp.concatenate([ref[here, pl.ds(a * width, width)] for a in range(heads)], 0)


def value_kernel(
    block,
    chosen_ref,
    queries_ref,
    out_grad_ref,
    sums_ref,
    own_ref,
    two_ref,
    four_ref,
    peer_ref,
    peer_two_ref,
    peer_four_ref,
    value_acc,
    value_low_ref,
    score_grads_ref,
    keys_ref,
    values,
    key_rows,
    value_rows,
):
    width = keys_ref.shape[2]
    heads = queries_ref.shape[1] // width
    blocks = queries_ref.shape[0] // block
    slots = chosen_ref.shape[2]
    scaling = width ** (-0.5)
    device = lax.axis_index("kv")
    odd = lax.rem(device, 2)

    def place(position, ref):
        for b in range(blocks):
            keys_ref[position * blocks + b] = ref[pl.ds(b * block, block), :width]
            values[position * blocks + b] = ref[pl.ds(b * block, block), width:]

    for back, (mine, theirs) in enumerate(
        ((own_ref, peer_ref), (two_ref, peer_two_ref), (four_ref, peer_four_ref))
    ):
        place(REACH - 2 * back + odd, mine)
        place(REACH - 2 * back + 1 - odd, theirs)

    value_acc[...] = jnp.zeros_like(value_acc)
    rows = heads * block
    key_pos = lax.broadcasted_iota(jnp.int32, (block, rows), 0)
    query_pos = lax.rem(lax.broadcasted_iota(jnp.int32, (block, rows), 1), block)
    causal = key_pos <= query_pos
    for b in range(blocks):
        here = pl.ds(b * block, block)
        places, listed = places_of(chosen_ref, b, blocks)
        offsets = [jnp.where(c < device * blocks + b, 0.0, 1e30) for c in listed] + [0.0]
        for s in range(slots + 1):
            key_rows[pl.ds(s * block, block), :] = keys_ref[places[s]]
            value_rows[pl.ds(s * block, block), :] = values[places[s]]
        q = stacked(queries_ref, b, block, width)
        g = stacked(out_grad_ref, b, block, width)
        sums = jnp.concatenate([sums_ref[pl.ds(a, 1), here] for a in range(heads)], 1) * LOG2E
        scores = lax.dot_general(
            key_rows[...], q, (((1,), (1,)), ((), ())), preferred_element_type=jnp.float32
        )
        grads = lax.dot_general(
            value_rows[...], g, (((1,), (1,)), ((), ())), preferred_element_type=jnp.float32
        )
        weights = []
        delta = jnp.zeros((1, rows), jnp.float32)
        for s in range(slots + 1):
            part = slice(s * block, (s + 1) * block)
            weight = jnp.exp2(scores[part] * (scaling * LOG2E) - (sums + offsets[s]))
            if s == slots:
                weight = jnp.where(causal, weight, 0.0)
            weights.append(weight)
            delta = delta + jnp.sum(weight * grads[part], 0, keepdims=True)
        for s in range(slots + 1):
            part = slice(s * block, (s + 1) * block)
            score_grad = weights[s] * (grads[part] - delta)
            score_grads_ref[b, pl.ds(s * block, block), :] = score_grad.astype(jnp.bfloat16)
        low = jnp.concatenate([w.astype(jnp.bfloat16) for w in weights], 0)
        value_part = jnp.dot(low, g, preferred_element_type=jnp.float32)
        for s in range(slots + 1):
            value_acc[places[s]] += value_part[s * block : (s + 1) * block]
    hand_over(value_acc, value_low_ref)


def key_kernel(
    block,
    chosen_ref,
    queries_ref,
    score_grads_ref,
    keys_ref,
    query_grad_ref,
    key_acc,
    key_low_ref,
    key_rows,
):
    width = keys_ref.shape[2]
    heads = queries_ref.shape[1] // width
    blocks = queries_ref.shape[0] // block
    scaling = width ** (-0.5)
    key_acc[...] = jnp.zeros_like(key_acc)
    for b in range(blocks):
        places, _ = places_of(chosen_ref, b, blocks)
        for s, position in enumerate(places):
            key_rows[pl.ds(s * block, block), :] = keys_ref[position]
        score_grads = score_grads_ref[b]
        q = stacked(queries_ref, b, block, width)
        key_part = jnp.dot(score_grads, q, preferred_element_type=jnp.float32) * scaling
        query_part = lax.dot_general(
            score_grads, key_rows[...], (((0,), (0,)), ((), ())), preferred_element_type=jnp.float32
        )
        for a in range(heads):
            query_grad_ref[pl.ds(b * block, block), pl.ds(a * width, width)] = (
                query_part[a * block : (a + 1) * block] * scaling
            ).astype(jnp.bfloat16)
        for s, position in enumerate(places):
            key_acc[position] += key_part[s * block : (s + 1) * block]
    hand_over(key_acc, key_low_ref)


def hand_over(acc_ref, low_ref):
    half = low_ref.shape[0] // 2
    odd = lax.rem(lax.axis_index("kv"), 2)
    low_ref[:half] = acc_ref[pl.ds(odd * half, half)].astype(jnp.bfloat16)
    low_ref[half:] = acc_ref[2 * half :].astype(jnp.bfloat16)


def chip_sum_kernel(mine_ref, came_ref, own_ref, send_ref):
    half = own_ref.shape[0]
    odd = lax.rem(lax.axis_index("kv"), 2)
    own_ref[...] = mine_ref[2 * half :] + came_ref[half:].astype(jnp.float32)
    total = mine_ref[pl.ds((1 - odd) * half, half)] + came_ref[:half].astype(jnp.float32)
    send_ref[...] = total.astype(jnp.bfloat16)


def total_kernel(own_ref, back_ref, other_ref, *refs):
    grad_ref = refs[-1]
    half = own_ref.shape[0] // 2
    odd = lax.rem(lax.axis_index("kv"), 2)

    def total(part):
        add = back_ref[part].astype(jnp.float32) + other_ref[part].astype(jnp.float32)
        return (own_ref[part] + add).astype(jnp.bfloat16)

    if len(refs) > 1:
        refs[0][...] = total(slice(None)).reshape(refs[0].shape)
    grad_ref[...] = total(pl.ds(odd * half, half)).reshape(grad_ref.shape)


def pair_kernel(keys_ref, values_ref, inputs_ref, pair_ref, rows_ref, done):
    width = keys_ref.shape[1]
    copies = [
        pltpu.make_async_copy(source, target, done.at[i])
        for i, (source, target) in enumerate(
            (
                (keys_ref, pair_ref.at[:, pl.ds(0, width)]),
                (values_ref, pair_ref.at[:, pl.ds(width, width)]),
                (inputs_ref, rows_ref),
            )
        )
    ]
    for copy in copies:
        copy.start()
    for copy in copies:
        copy.wait()


def select_kernel(odd_ref, even_ref, out_ref):
    odd = lax.rem(lax.axis_index("kv") // 4, 2)

    @pl.when(odd == 1)
    def _():
        out_ref[...] = odd_ref[...]

    @pl.when(odd == 0)
    def _():
        out_ref[...] = even_ref[...]


def transpose_kernel(piece, rows_ref, keep_ref, give_ref, turned_rows):
    turned_rows[...] = rows_ref[...].T
    corner = lax.rem(lax.axis_index("kv"), 4)
    for i in range(2):
        for out, owner in ((keep_ref, corner ^ (2 * i)), (give_ref, corner ^ (2 * i + 1))):
            for group in range(out.shape[1] // piece):
                out[i, pl.ds(group * piece, piece), :] = turned_rows[
                    pl.ds((4 * group + owner) * piece, piece), :
                ]


def join_kernel(keep_ref, got_ref, own_ref, across_ref):
    tokens = keep_ref.shape[2]
    odd = lax.rem(lax.axis_index("kv"), 2)
    for i, out in enumerate((own_ref, across_ref)):
        out[:, pl.ds(pl.multiple_of(odd * tokens, tokens), tokens)] = keep_ref[i]
        out[:, pl.ds(pl.multiple_of((1 - odd) * tokens, tokens), tokens)] = got_ref[i]


def partner(digit, step, radix):
    if radix & (radix - 1):
        return lax.rem(digit + step, radix)
    return digit ^ step


def product_kernel(shares, grads_ref, *refs):
    factors, out = refs[:shares], refs[shares]
    piece = out.shape[1]
    per_share = factors[0].shape[0] // piece
    part = lax.axis_index("tp")
    for step in range(shares):
        where = lax.rem(part + shares - step, shares)
        total = jnp.dot(factors[step][...], grads_ref[...], preferred_element_type=jnp.float32)
        for i in range(per_share):
            out[where * per_share + i] = total[i * piece : (i + 1) * piece].astype(out.dtype)


def spread_kernel(stride, radix, keep_ref, came_ref, *outs):
    mine_ref, sends = outs[0], outs[1:]
    digit = lax.rem(lax.axis_index("kv") // stride, radix)
    for i in range(mine_ref.shape[0]):
        at = radix * i + digit
        mine_ref[i] = keep_ref[at] + came_ref[at].astype(jnp.float32)
        for s, send in enumerate(sends):
            at = radix * i + partner(digit, s + 1, radix)
            send[i] = (keep_ref[at] + came_ref[at].astype(jnp.float32)).astype(jnp.bfloat16)


def spread(kept, came, stride, radix):
    shape = (kept.shape[0] // radix,) + kept.shape[1:]
    return pl.pallas_call(
        functools.partial(spread_kernel, stride, radix),
        out_shape=[pltpu.VMEM(shape, jnp.float32)] + [pltpu.VMEM(shape, jnp.bfloat16)] * (radix - 1),
        in_specs=vmem(2),
        out_specs=vmem(radix),
        compiler_params=PARAMS,
    )(*near(kept, came))


def radices(count):
    found = []
    for radix in (4, 3, 2):
        while count % radix == 0:
            found.append(radix)
            count //= radix
    if count > 1:
        found.append(count)
    return found


def shards(queries, keys, values, log_sums, out_grad, chosen, inputs):
    tokens, width = keys.shape
    blocks = chosen.shape[0]
    block = tokens // blocks
    heads = queries.shape[1] // width
    slots = chosen.shape[2]
    count = lax.axis_size("kv")
    shares = lax.axis_size("tp")
    features = inputs.shape[1]
    piece = features * shares // count
    window = (REACH + 2) * blocks
    bf16, f32 = jnp.bfloat16, jnp.float32

    pair, rows = pl.pallas_call(
        pair_kernel,
        out_shape=[pltpu.VMEM((tokens, 2 * width), bf16), pltpu.VMEM(inputs.shape, bf16)],
        in_specs=[pl.BlockSpec(memory_space=pltpu.HBM)] * 3,
        out_specs=vmem(2),
        scratch_shapes=[pltpu.SemaphoreType.DMA((3,))],
        compiler_params=PARAMS,
    )(*far(keys, values, inputs))
    four_odd = exchanged(pair, 0)
    four_even = exchanged(pair, 1)
    four = pl.pallas_call(
        select_kernel,
        out_shape=pltpu.VMEM(pair.shape, bf16),
        in_specs=vmem(2),
        out_specs=pl.BlockSpec(memory_space=pltpu.VMEM),
        compiler_params=PARAMS,
    )(*near(four_odd, four_even))
    two = shifted(pair, 2)
    peer = swapped(pair, 1)
    peer_four = swapped(four, 1)
    peer_two = swapped(two, 1)

    keep, give = pl.pallas_call(
        functools.partial(transpose_kernel, piece),
        out_shape=[pltpu.VMEM((2, features // 4, tokens), bf16)] * 2,
        in_specs=vmem(1),
        out_specs=vmem(2),
        scratch_shapes=[pltpu.VMEM((features, tokens), bf16)],
        compiler_params=PARAMS,
    )(*near(rows))
    got = swapped(give, 1)
    own_factor, across = pl.pallas_call(
        join_kernel,
        out_shape=[pltpu.VMEM((features // 4, 2 * tokens), bf16)] * 2,
        in_specs=vmem(2),
        out_specs=vmem(2),
        compiler_params=PARAMS,
    )(*near(keep, got))
    own_factors, across_factors = [own_factor], [across]
    for step in range(1, shares):
        pairs = [(i, (i + step) % shares) for i in range(shares)]
        across_factors.append(lax.ppermute(across, "tp", pairs))
        own_factors.append(lax.ppermute(own_factor, "tp", pairs))

    queries, out_grad, log_sums = near(queries, out_grad, log_sums)
    value_acc, value_low, score_grads, window_keys = pl.pallas_call(
        functools.partial(value_kernel, block),
        out_shape=[
            pltpu.VMEM((window, block, width), f32),
            pltpu.VMEM((4 * blocks, block, width), bf16),
            pltpu.VMEM((blocks, (slots + 1) * block, heads * block), bf16),
            pltpu.VMEM((window, block, width), bf16),
        ],
        in_specs=[pl.BlockSpec(memory_space=pltpu.SMEM)] + vmem(9),
        out_specs=vmem(4),
        scratch_shapes=[
            pltpu.VMEM((window, block, width), bf16),
            pltpu.VMEM(((slots + 1) * block, width), bf16),
            pltpu.VMEM(((slots + 1) * block, width), bf16),
        ],
        compiler_params=PARAMS,
    )(
        chosen,
        queries,
        out_grad,
        log_sums,
        *near(pair, two, four, peer, peer_two, peer_four),
    )
    query_grad, key_acc, key_low = pl.pallas_call(
        functools.partial(key_kernel, block),
        out_shape=[
            pltpu.VMEM(queries.shape, bf16),
            pltpu.VMEM((window, block, width), f32),
            pltpu.VMEM((4 * blocks, block, width), bf16),
        ],
        in_specs=[pl.BlockSpec(memory_space=pltpu.SMEM)] + vmem(3),
        out_specs=vmem(3),
        scratch_shapes=[pltpu.VMEM(((slots + 1) * block, width), bf16)],
        compiler_params=PARAMS,
    )(chosen, queries, *near(score_grads, window_keys))

    def gathered(acc, low, both):
        came = swapped(low, 1)
        own, send = pl.pallas_call(
            chip_sum_kernel,
            out_shape=[
                pltpu.VMEM((2 * blocks, block, width), f32),
                pltpu.VMEM((2 * blocks, block, width), bf16),
            ],
            in_specs=vmem(2),
            out_specs=vmem(2),
            compiler_params=PARAMS,
        )(*near(acc, came))
        back = returned(send)
        other = swapped(back, 1)
        return pl.pallas_call(
            total_kernel,
            out_shape=[pltpu.VMEM((2 * tokens, width), bf16)] * both
            + [pltpu.VMEM((tokens, width), bf16)],
            in_specs=vmem(3),
            out_specs=vmem(both + 1),
            compiler_params=PARAMS,
        )(*near(own, back, other))

    value_both, value_grad = gathered(value_acc, value_low, 1)
    (key_grad,) = gathered(key_acc, key_low, 0)

    pieces = count // 4

    def product(factors, dtype):
        return pl.pallas_call(
            functools.partial(product_kernel, shares),
            out_shape=pltpu.VMEM((pieces, piece, width), dtype),
            in_specs=vmem(1 + shares),
            out_specs=pl.BlockSpec(memory_space=pltpu.VMEM),
            compiler_params=PARAMS,
        )(*near(value_both, *factors))

    sent = product(across_factors, bf16)
    came = swapped(sent, 2)
    kept = product(own_factors, f32)
    stride = 4
    for radix in radices(pieces):
        kept, *sends = spread(kept, came, stride, radix)
        came = 0.0
        for s, send in enumerate(sends):
            came = came + turned(send, stride, radix, s + 1).astype(f32)
        stride *= radix
    weight_grad = (kept + came)[0]
    return (query_grad, key_grad, value_grad, weight_grad)


def solution(mesh):
    in_specs = (
        P("kv", "tp"),
        P("kv", "tp"),
        P("kv", "tp"),
        P("tp", "kv"),
        P("kv", "tp"),
        P("kv", "tp", None),
        P("kv", "tp"),
    )
    out_specs = (P("kv", "tp"), P("kv", "tp"), P("kv", "tp"), P("kv", "tp"))

    return jax.shard_map(shards, mesh=mesh, in_specs=in_specs, out_specs=out_specs, check_vma=False)
```

```python
import functools

import jax
import jax.numpy as jnp
from jax import lax
from jax.experimental import pallas as pl
from jax.experimental.pallas import tpu as pltpu
from jax.sharding import PartitionSpec as P


REACH = 4
LOG2E = 1.4426950408889634


PARAMS = pltpu.CompilerParams(vmem_limit_bytes=24 << 20)


def vmem(count):
    return [pl.BlockSpec(memory_space=pltpu.VMEM)] * count


def near(*values):
    return [pltpu.with_memory_space_constraint(v, pltpu.VMEM) for v in values]


def far(*values):
    return [pltpu.with_memory_space_constraint(v, pltpu.HBM) for v in values]


def shifted(value, steps):
    count = lax.axis_size("kv")
    return lax.ppermute(value, "kv", [(i, (i + steps) % count) for i in range(count)])


def returned(value):
    count = lax.axis_size("kv")
    moves = [(i, (i - (4 if i % 2 else 2)) % count) for i in range(count)]
    return lax.ppermute(value, "kv", moves)


def swapped(value, bit):
    count = lax.axis_size("kv")
    return lax.ppermute(value, "kv", [(i, i ^ bit) for i in range(count)])


def turned(value, stride, radix, steps):
    count = lax.axis_size("kv")
    pairs = []
    for i in range(count):
        digit = i // stride % radix
        target = (digit + steps) % radix if radix & (radix - 1) else digit ^ steps
        pairs.append((i, i + (target - digit) * stride))
    return lax.ppermute(value, "kv", pairs)


def places_of(chosen_ref, b, blocks):
    device = lax.axis_index("kv")
    odd = lax.rem(device, 2)
    first = (device - odd - REACH) * blocks
    listed = [chosen_ref[b, 0, s] for s in range(chosen_ref.shape[2])]
    return [c - first for c in listed] + [(REACH + odd) * blocks + b], listed


def stacked(ref, b, block, width):
    heads = ref.shape[1] // width
    here = pl.ds(b * block, block)
    return jnp.concatenate([ref[here, pl.ds(a * width, width)] for a in range(heads)], 0)


def value_kernel(
    block,
    chosen_ref,
    queries_ref,
    out_grad_ref,
    sums_ref,
    own_ref,
    two_ref,
    four_ref,
    peer_ref,
    peer_two_ref,
    peer_four_ref,
    value_acc,
    value_low_ref,
    weights_ref,
    window,
    key_rows,
):
    width = window.shape[2] // 2
    heads = queries_ref.shape[1] // width
    blocks = queries_ref.shape[0] // block
    slots = chosen_ref.shape[2]
    scaling = width ** (-0.5)
    device = lax.axis_index("kv")
    odd = lax.rem(device, 2)

    def place(position, ref):
        for b in range(blocks):
            window[position * blocks + b] = ref[pl.ds(b * block, block), :]

    for back, (mine, theirs) in enumerate(
        ((own_ref, peer_ref), (two_ref, peer_two_ref), (four_ref, peer_four_ref))
    ):
        place(REACH - 2 * back + odd, mine)
        place(REACH - 2 * back + 1 - odd, theirs)

    value_acc[...] = jnp.zeros_like(value_acc)
    rows = heads * block
    key_pos = lax.broadcasted_iota(jnp.int32, (block, rows), 0)
    query_pos = lax.rem(lax.broadcasted_iota(jnp.int32, (block, rows), 1), block)
    causal = key_pos <= query_pos
    for b in range(blocks):
        here = pl.ds(b * block, block)
        places, listed = places_of(chosen_ref, b, blocks)
        offsets = [jnp.where(c < device * blocks + b, 0.0, 1e30) for c in listed] + [0.0]
        for s in range(slots + 1):
            key_rows[pl.ds(s * block, block), :] = window[places[s], :, :width]
        q = stacked(queries_ref, b, block, width)
        g = stacked(out_grad_ref, b, block, width)
        sums = jnp.concatenate([sums_ref[pl.ds(a, 1), here] for a in range(heads)], 1) * LOG2E
        scores = lax.dot_general(
            key_rows[...], q, (((1,), (1,)), ((), ())), preferred_element_type=jnp.float32
        )
        low = []
        for s in range(slots + 1):
            part = slice(s * block, (s + 1) * block)
            weight = jnp.exp2(scores[part] * (scaling * LOG2E) - (sums + offsets[s]))
            if s == slots:
                weight = jnp.where(causal, weight, 0.0)
            weights_ref[b, pl.ds(s * block, block), :] = weight
            low.append(weight.astype(jnp.bfloat16))
        value_part = jnp.dot(jnp.concatenate(low, 0), g, preferred_element_type=jnp.float32)
        for s in range(slots + 1):
            value_acc[places[s]] += value_part[s * block : (s + 1) * block]
    hand_over(value_acc, value_low_ref)


def key_kernel(
    block,
    chosen_ref,
    queries_ref,
    out_grad_ref,
    weights_ref,
    window,
    query_grad_ref,
    key_acc,
    key_low_ref,
    key_rows,
    value_rows,
):
    width = window.shape[2] // 2
    heads = queries_ref.shape[1] // width
    blocks = queries_ref.shape[0] // block
    scaling = width ** (-0.5)
    key_acc[...] = jnp.zeros_like(key_acc)
    for b in range(blocks):
        places, _ = places_of(chosen_ref, b, blocks)
        for s, position in enumerate(places):
            key_rows[pl.ds(s * block, block), :] = window[position, :, :width]
            value_rows[pl.ds(s * block, block), :] = window[position, :, width:]
        q = stacked(queries_ref, b, block, width)
        g = stacked(out_grad_ref, b, block, width)
        grads = lax.dot_general(
            value_rows[...], g, (((1,), (1,)), ((), ())), preferred_element_type=jnp.float32
        )
        weights = weights_ref[b]
        delta = jnp.sum(weights * grads, 0, keepdims=True)
        score_grads = (weights * (grads - delta)).astype(jnp.bfloat16)
        key_part = jnp.dot(score_grads, q, preferred_element_type=jnp.float32) * scaling
        query_part = lax.dot_general(
            score_grads, key_rows[...], (((0,), (0,)), ((), ())), preferred_element_type=jnp.float32
        )
        for a in range(heads):
            query_grad_ref[pl.ds(b * block, block), pl.ds(a * width, width)] = (
                query_part[a * block : (a + 1) * block] * scaling
            ).astype(jnp.bfloat16)
        for s, position in enumerate(places):
            key_acc[position] += key_part[s * block : (s + 1) * block]
    hand_over(key_acc, key_low_ref)


def hand_over(acc_ref, low_ref):
    half = low_ref.shape[0] // 2
    odd = lax.rem(lax.axis_index("kv"), 2)
    low_ref[:half] = acc_ref[pl.ds(odd * half, half)].astype(jnp.bfloat16)
    low_ref[half:] = acc_ref[2 * half :].astype(jnp.bfloat16)


def chip_sum_kernel(mine_ref, came_ref, own_ref, send_ref):
    half = own_ref.shape[0]
    odd = lax.rem(lax.axis_index("kv"), 2)
    own_ref[...] = mine_ref[2 * half :] + came_ref[half:].astype(jnp.float32)
    total = mine_ref[pl.ds((1 - odd) * half, half)] + came_ref[:half].astype(jnp.float32)
    send_ref[...] = total.astype(jnp.bfloat16)


def total_kernel(own_ref, back_ref, other_ref, *refs):
    grad_ref = refs[-1]
    half = own_ref.shape[0] // 2
    odd = lax.rem(lax.axis_index("kv"), 2)

    def total(part):
        add = back_ref[part].astype(jnp.float32) + other_ref[part].astype(jnp.float32)
        return (own_ref[part] + add).astype(jnp.bfloat16)

    if len(refs) > 1:
        refs[0][...] = total(slice(None)).reshape(refs[0].shape)
    grad_ref[...] = total(pl.ds(odd * half, half)).reshape(grad_ref.shape)


def pair_kernel(keys_ref, values_ref, inputs_ref, pair_ref, rows_ref, done):
    width = keys_ref.shape[1]
    copies = [
        pltpu.make_async_copy(source, target, done.at[i])
        for i, (source, target) in enumerate(
            (
                (keys_ref, pair_ref.at[:, pl.ds(0, width)]),
                (values_ref, pair_ref.at[:, pl.ds(width, width)]),
                (inputs_ref, rows_ref),
            )
        )
    ]
    for copy in copies:
        copy.start()
    for copy in copies:
        copy.wait()


def transpose_kernel(piece, rows_ref, keep_ref, give_ref, turned_rows):
    turned_rows[...] = rows_ref[...].T
    corner = lax.rem(lax.axis_index("kv"), 4)
    for i in range(2):
        for out, owner in ((keep_ref, corner ^ (2 * i)), (give_ref, corner ^ (2 * i + 1))):
            for group in range(out.shape[1] // piece):
                out[i, pl.ds(group * piece, piece), :] = turned_rows[
                    pl.ds((4 * group + owner) * piece, piece), :
                ]


def join_kernel(keep_ref, got_ref, own_ref, across_ref):
    tokens = keep_ref.shape[2]
    odd = lax.rem(lax.axis_index("kv"), 2)
    for i, out in enumerate((own_ref, across_ref)):
        out[:, pl.ds(pl.multiple_of(odd * tokens, tokens), tokens)] = keep_ref[i]
        out[:, pl.ds(pl.multiple_of((1 - odd) * tokens, tokens), tokens)] = got_ref[i]


def partner(digit, step, radix):
    if radix & (radix - 1):
        return lax.rem(digit + step, radix)
    return digit ^ step


def product_kernel(shares, grads_ref, *refs):
    factors, out = refs[:shares], refs[shares]
    piece = out.shape[1]
    per_share = factors[0].shape[0] // piece
    part = lax.axis_index("tp")
    for step in range(shares):
        where = lax.rem(part + shares - step, shares)
        total = jnp.dot(factors[step][...], grads_ref[...], preferred_element_type=jnp.float32)
        for i in range(per_share):
            out[where * per_share + i] = total[i * piece : (i + 1) * piece].astype(out.dtype)


def spread_kernel(stride, radix, keep_ref, came_ref, *outs):
    mine_ref, sends = outs[0], outs[1:]
    digit = lax.rem(lax.axis_index("kv") // stride, radix)
    for i in range(mine_ref.shape[0]):
        at = radix * i + digit
        mine_ref[i] = keep_ref[at] + came_ref[at].astype(jnp.float32)
        for s, send in enumerate(sends):
            at = radix * i + partner(digit, s + 1, radix)
            send[i] = (keep_ref[at] + came_ref[at].astype(jnp.float32)).astype(jnp.bfloat16)


def spread(kept, came, stride, radix):
    shape = (kept.shape[0] // radix,) + kept.shape[1:]
    return pl.pallas_call(
        functools.partial(spread_kernel, stride, radix),
        out_shape=[pltpu.VMEM(shape, jnp.float32)] + [pltpu.VMEM(shape, jnp.bfloat16)] * (radix - 1),
        in_specs=vmem(2),
        out_specs=vmem(radix),
        compiler_params=PARAMS,
    )(*near(kept, came))


def radices(count):
    found = []
    for radix in (4, 3, 2):
        while count % radix == 0:
            found.append(radix)
            count //= radix
    if count > 1:
        found.append(count)
    return found


def shards(queries, keys, values, log_sums, out_grad, chosen, inputs):
    tokens, width = keys.shape
    blocks = chosen.shape[0]
    block = tokens // blocks
    heads = queries.shape[1] // width
    slots = chosen.shape[2]
    count = lax.axis_size("kv")
    shares = lax.axis_size("tp")
    features = inputs.shape[1]
    piece = features * shares // count
    window = (REACH + 2) * blocks
    bf16, f32 = jnp.bfloat16, jnp.float32

    pair, rows = pl.pallas_call(
        pair_kernel,
        out_shape=[pltpu.VMEM((tokens, 2 * width), bf16), pltpu.VMEM(inputs.shape, bf16)],
        in_specs=[pl.BlockSpec(memory_space=pltpu.HBM)] * 3,
        out_specs=vmem(2),
        scratch_shapes=[pltpu.SemaphoreType.DMA((3,))],
        compiler_params=PARAMS,
    )(*far(keys, values, inputs))
    four = shifted(pair, 4)
    two = shifted(pair, 2)
    peer = swapped(pair, 1)
    peer_four = swapped(four, 1)
    peer_two = swapped(two, 1)

    keep, give = pl.pallas_call(
        functools.partial(transpose_kernel, piece),
        out_shape=[pltpu.VMEM((2, features // 4, tokens), bf16)] * 2,
        in_specs=vmem(1),
        out_specs=vmem(2),
        scratch_shapes=[pltpu.VMEM((features, tokens), bf16)],
        compiler_params=PARAMS,
    )(*near(rows))
    got = swapped(give, 1)
    own_factor, across = pl.pallas_call(
        join_kernel,
        out_shape=[pltpu.VMEM((features // 4, 2 * tokens), bf16)] * 2,
        in_specs=vmem(2),
        out_specs=vmem(2),
        compiler_params=PARAMS,
    )(*near(keep, got))
    own_factors, across_factors = [own_factor], [across]
    for step in range(1, shares):
        pairs = [(i, (i + step) % shares) for i in range(shares)]
        across_factors.append(lax.ppermute(across, "tp", pairs))
        own_factors.append(lax.ppermute(own_factor, "tp", pairs))

    queries, out_grad, log_sums = near(queries, out_grad, log_sums)
    value_acc, value_low, weights, key_values = pl.pallas_call(
        functools.partial(value_kernel, block),
        out_shape=[
            pltpu.VMEM((window, block, width), f32),
            pltpu.VMEM((4 * blocks, block, width), bf16),
            pltpu.VMEM((blocks, (slots + 1) * block, heads * block), f32),
            pltpu.VMEM((window, block, 2 * width), bf16),
        ],
        in_specs=[pl.BlockSpec(memory_space=pltpu.SMEM)] + vmem(9),
        out_specs=vmem(4),
        scratch_shapes=[pltpu.VMEM(((slots + 1) * block, width), bf16)],
        compiler_params=PARAMS,
    )(
        chosen,
        queries,
        out_grad,
        log_sums,
        *near(pair, two, four, peer, peer_two, peer_four),
    )
    query_grad, key_acc, key_low = pl.pallas_call(
        functools.partial(key_kernel, block),
        out_shape=[
            pltpu.VMEM(queries.shape, bf16),
            pltpu.VMEM((window, block, width), f32),
            pltpu.VMEM((4 * blocks, block, width), bf16),
        ],
        in_specs=[pl.BlockSpec(memory_space=pltpu.SMEM)] + vmem(4),
        out_specs=vmem(3),
        scratch_shapes=[pltpu.VMEM(((slots + 1) * block, width), bf16)] * 2,
        compiler_params=PARAMS,
    )(chosen, queries, out_grad, *near(weights, key_values))

    def gathered(acc, low, both):
        came = swapped(low, 1)
        own, send = pl.pallas_call(
            chip_sum_kernel,
            out_shape=[
                pltpu.VMEM((2 * blocks, block, width), f32),
                pltpu.VMEM((2 * blocks, block, width), bf16),
            ],
            in_specs=vmem(2),
            out_specs=vmem(2),
            compiler_params=PARAMS,
        )(*near(acc, came))
        back = returned(send)
        other = swapped(back, 1)
        return pl.pallas_call(
            total_kernel,
            out_shape=[pltpu.VMEM((2 * tokens, width), bf16)] * both
            + [pltpu.VMEM((tokens, width), bf16)],
            in_specs=vmem(3),
            out_specs=vmem(both + 1),
            compiler_params=PARAMS,
        )(*near(own, back, other))

    value_both, value_grad = gathered(value_acc, value_low, 1)
    (key_grad,) = gathered(key_acc, key_low, 0)

    pieces = count // 4

    def product(factors, dtype):
        return pl.pallas_call(
            functools.partial(product_kernel, shares),
            out_shape=pltpu.VMEM((pieces, piece, width), dtype),
            in_specs=vmem(1 + shares),
            out_specs=pl.BlockSpec(memory_space=pltpu.VMEM),
            compiler_params=PARAMS,
        )(*near(value_both, *factors))

    sent = product(across_factors, bf16)
    came = swapped(sent, 2)
    kept = product(own_factors, f32)
    stride = 4
    for radix in radices(pieces):
        kept, *sends = spread(kept, came, stride, radix)
        came = 0.0
        for s, send in enumerate(sends):
            came = came + turned(send, stride, radix, s + 1).astype(f32)
        stride *= radix
    weight_grad = (kept + came)[0]
    return (query_grad, key_grad, value_grad, weight_grad)


def solution(mesh):
    in_specs = (
        P("kv", "tp"),
        P("kv", "tp"),
        P("kv", "tp"),
        P("tp", "kv"),
        P("kv", "tp"),
        P("kv", "tp", None),
        P("kv", "tp"),
    )
    out_specs = (P("kv", "tp"), P("kv", "tp"), P("kv", "tp"), P("kv", "tp"))

    return jax.shard_map(shards, mesh=mesh, in_specs=in_specs, out_specs=out_specs, check_vma=False)
```

```python
import functools

import jax
import jax.numpy as jnp
from jax import lax
from jax.experimental import pallas as pl
from jax.experimental.pallas import tpu as pltpu
from jax.sharding import PartitionSpec as P


REACH = 4
LOG2E = 1.4426950408889634


PARAMS = pltpu.CompilerParams(vmem_limit_bytes=24 << 20)


def vmem(count):
    return [pl.BlockSpec(memory_space=pltpu.VMEM)] * count


def near(*values):
    return [pltpu.with_memory_space_constraint(v, pltpu.VMEM) for v in values]


def far(*values):
    return [pltpu.with_memory_space_constraint(v, pltpu.HBM) for v in values]


def shifted(value, steps):
    count = lax.axis_size("kv")
    return lax.ppermute(value, "kv", [(i, (i + steps) % count) for i in range(count)])


def returned(value):
    count = lax.axis_size("kv")
    moves = [(i, (i - (4 if i % 2 else 2)) % count) for i in range(count)]
    return lax.ppermute(value, "kv", moves)


def swapped(value, bit):
    count = lax.axis_size("kv")
    return lax.ppermute(value, "kv", [(i, i ^ bit) for i in range(count)])


def turned(value, stride, radix, steps):
    count = lax.axis_size("kv")
    pairs = []
    for i in range(count):
        digit = i // stride % radix
        target = (digit + steps) % radix if radix & (radix - 1) else digit ^ steps
        pairs.append((i, i + (target - digit) * stride))
    return lax.ppermute(value, "kv", pairs)


def places_of(chosen_ref, b, blocks):
    device = lax.axis_index("kv")
    odd = lax.rem(device, 2)
    first = (device - odd - REACH) * blocks
    listed = [chosen_ref[b, 0, s] for s in range(chosen_ref.shape[2])]
    return [c - first for c in listed] + [(REACH + odd) * blocks + b], listed


def stacked(ref, b, block, width):
    heads = ref.shape[1] // width
    here = pl.ds(b * block, block)
    return jnp.concatenate([ref[here, pl.ds(a * width, width)] for a in range(heads)], 0)


def value_kernel(
    block,
    chosen_ref,
    queries_ref,
    out_grad_ref,
    sums_ref,
    own_ref,
    two_ref,
    four_ref,
    peer_ref,
    peer_two_ref,
    peer_four_ref,
    value_acc,
    value_low_ref,
    weights_ref,
    window,
    key_rows,
):
    width = window.shape[2] // 2
    heads = queries_ref.shape[1] // width
    blocks = queries_ref.shape[0] // block
    slots = chosen_ref.shape[2]
    scaling = width ** (-0.5)
    device = lax.axis_index("kv")
    odd = lax.rem(device, 2)

    def place(position, ref):
        for b in range(blocks):
            window[position * blocks + b] = ref[pl.ds(b * block, block), :]

    for back, (mine, theirs) in enumerate(
        ((own_ref, peer_ref), (two_ref, peer_two_ref), (four_ref, peer_four_ref))
    ):
        place(REACH - 2 * back + odd, mine)
        place(REACH - 2 * back + 1 - odd, theirs)

    value_acc[...] = jnp.zeros_like(value_acc)
    rows = heads * block
    key_pos = lax.broadcasted_iota(jnp.int32, (block, rows), 0)
    query_pos = lax.rem(lax.broadcasted_iota(jnp.int32, (block, rows), 1), block)
    causal = key_pos <= query_pos
    for b in range(blocks):
        here = pl.ds(b * block, block)
        places, listed = places_of(chosen_ref, b, blocks)
        offsets = [jnp.where(c < device * blocks + b, 0.0, 1e30) for c in listed] + [0.0]
        for s in range(slots + 1):
            key_rows[pl.ds(s * block, block), :] = window[places[s], :, :width]
        q = stacked(queries_ref, b, block, width)
        g = stacked(out_grad_ref, b, block, width)
        sums = jnp.concatenate([sums_ref[pl.ds(a, 1), here] for a in range(heads)], 1) * LOG2E
        scores = lax.dot_general(
            key_rows[...], q, (((1,), (1,)), ((), ())), preferred_element_type=jnp.float32
        )
        low = []
        for s in range(slots + 1):
            part = slice(s * block, (s + 1) * block)
            weight = jnp.exp2(scores[part] * (scaling * LOG2E) - (sums + offsets[s]))
            if s == slots:
                weight = jnp.where(causal, weight, 0.0)
            weights_ref[b, pl.ds(s * block, block), :] = weight
            low.append(weight.astype(jnp.bfloat16))
        value_part = jnp.dot(jnp.concatenate(low, 0), g, preferred_element_type=jnp.float32)
        for s in range(slots + 1):
            value_acc[places[s]] += value_part[s * block : (s + 1) * block]
    hand_over(value_acc, value_low_ref)


def key_kernel(
    block,
    chosen_ref,
    queries_ref,
    out_grad_ref,
    weights_ref,
    window,
    query_grad_ref,
    key_acc,
    key_low_ref,
    key_rows,
    value_rows,
):
    width = window.shape[2] // 2
    heads = queries_ref.shape[1] // width
    blocks = queries_ref.shape[0] // block
    scaling = width ** (-0.5)
    key_acc[...] = jnp.zeros_like(key_acc)
    for b in range(blocks):
        places, _ = places_of(chosen_ref, b, blocks)
        for s, position in enumerate(places):
            key_rows[pl.ds(s * block, block), :] = window[position, :, :width]
            value_rows[pl.ds(s * block, block), :] = window[position, :, width:]
        q = stacked(queries_ref, b, block, width)
        g = stacked(out_grad_ref, b, block, width)
        grads = lax.dot_general(
            value_rows[...], g, (((1,), (1,)), ((), ())), preferred_element_type=jnp.float32
        )
        weights = weights_ref[b]
        delta = jnp.sum(weights * grads, 0, keepdims=True)
        score_grads = (weights * (grads - delta)).astype(jnp.bfloat16)
        key_part = jnp.dot(score_grads, q, preferred_element_type=jnp.float32) * scaling
        query_part = lax.dot_general(
            score_grads, key_rows[...], (((0,), (0,)), ((), ())), preferred_element_type=jnp.float32
        )
        for a in range(heads):
            query_grad_ref[pl.ds(b * block, block), pl.ds(a * width, width)] = (
                query_part[a * block : (a + 1) * block] * scaling
            ).astype(jnp.bfloat16)
        for s, position in enumerate(places):
            key_acc[position] += key_part[s * block : (s + 1) * block]
    hand_over(key_acc, key_low_ref)


def hand_over(acc_ref, low_ref):
    half = low_ref.shape[0] // 2
    odd = lax.rem(lax.axis_index("kv"), 2)
    low_ref[:half] = acc_ref[pl.ds(odd * half, half)].astype(jnp.bfloat16)
    low_ref[half:] = acc_ref[2 * half :].astype(jnp.bfloat16)


def chip_sum_kernel(mine_ref, came_ref, own_ref, send_ref):
    half = own_ref.shape[0]
    odd = lax.rem(lax.axis_index("kv"), 2)
    own_ref[...] = mine_ref[2 * half :] + came_ref[half:].astype(jnp.float32)
    total = mine_ref[pl.ds((1 - odd) * half, half)] + came_ref[:half].astype(jnp.float32)
    send_ref[...] = total.astype(jnp.bfloat16)


def total_kernel(own_ref, back_ref, other_ref, *refs):
    grad_ref = refs[-1]
    half = own_ref.shape[0] // 2
    odd = lax.rem(lax.axis_index("kv"), 2)

    def total(part):
        add = back_ref[part].astype(jnp.float32) + other_ref[part].astype(jnp.float32)
        return (own_ref[part] + add).astype(jnp.bfloat16)

    if len(refs) > 1:
        refs[0][...] = total(slice(None)).reshape(refs[0].shape)
    grad_ref[...] = total(pl.ds(odd * half, half)).reshape(grad_ref.shape)


def bring(pairs, done):
    copies = [pltpu.make_async_copy(a, b, done.at[i]) for i, (a, b) in enumerate(pairs)]
    for copy in copies:
        copy.start()
    for copy in copies:
        copy.wait()


def pair_kernel(keys_ref, values_ref, pair_ref, done):
    width = keys_ref.shape[1]
    left, right = pair_ref.at[:, pl.ds(0, width)], pair_ref.at[:, pl.ds(width, width)]
    bring([(keys_ref, left), (values_ref, right)], done)


def fetch_kernel(*refs):
    half = len(refs) // 2
    bring(list(zip(refs[:half], refs[half:-1])), refs[-1])


def transpose_kernel(piece, inputs_ref, keep_ref, give_ref, rows, turned_rows, done):
    bring([(inputs_ref, rows)], done)
    turned_rows[...] = rows[...].T
    corner = lax.rem(lax.axis_index("kv"), 4)
    for i in range(2):
        for out, owner in ((keep_ref, corner ^ (2 * i)), (give_ref, corner ^ (2 * i + 1))):
            for group in range(out.shape[1] // piece):
                out[i, pl.ds(group * piece, piece), :] = turned_rows[
                    pl.ds((4 * group + owner) * piece, piece), :
                ]


def join_kernel(keep_ref, got_ref, own_ref, across_ref):
    tokens = keep_ref.shape[2]
    odd = lax.rem(lax.axis_index("kv"), 2)
    for i, out in enumerate((own_ref, across_ref)):
        out[:, pl.ds(pl.multiple_of(odd * tokens, tokens), tokens)] = keep_ref[i]
        out[:, pl.ds(pl.multiple_of((1 - odd) * tokens, tokens), tokens)] = got_ref[i]


def partner(digit, step, radix):
    if radix & (radix - 1):
        return lax.rem(digit + step, radix)
    return digit ^ step


def product_kernel(shares, grads_ref, *refs):
    factors, out = refs[:shares], refs[shares]
    piece = out.shape[1]
    per_share = factors[0].shape[0] // piece
    part = lax.axis_index("tp")
    for step in range(shares):
        where = lax.rem(part + shares - step, shares)
        total = jnp.dot(factors[step][...], grads_ref[...], preferred_element_type=jnp.float32)
        for i in range(per_share):
            out[where * per_share + i] = total[i * piece : (i + 1) * piece].astype(out.dtype)


def spread_kernel(stride, radix, keep_ref, came_ref, *outs):
    mine_ref, sends = outs[0], outs[1:]
    digit = lax.rem(lax.axis_index("kv") // stride, radix)
    for i in range(mine_ref.shape[0]):
        at = radix * i + digit
        mine_ref[i] = keep_ref[at] + came_ref[at].astype(jnp.float32)
        for s, send in enumerate(sends):
            at = radix * i + partner(digit, s + 1, radix)
            send[i] = (keep_ref[at] + came_ref[at].astype(jnp.float32)).astype(jnp.bfloat16)


def spread(kept, came, stride, radix):
    shape = (kept.shape[0] // radix,) + kept.shape[1:]
    return pl.pallas_call(
        functools.partial(spread_kernel, stride, radix),
        out_shape=[pltpu.VMEM(shape, jnp.float32)] + [pltpu.VMEM(shape, jnp.bfloat16)] * (radix - 1),
        in_specs=vmem(2),
        out_specs=vmem(radix),
        compiler_params=PARAMS,
    )(*near(kept, came))


def radices(count):
    found = []
    for radix in (4, 3, 2):
        while count % radix == 0:
            found.append(radix)
            count //= radix
    if count > 1:
        found.append(count)
    return found


def shards(queries, keys, values, log_sums, out_grad, chosen, inputs):
    tokens, width = keys.shape
    blocks = chosen.shape[0]
    block = tokens // blocks
    heads = queries.shape[1] // width
    slots = chosen.shape[2]
    count = lax.axis_size("kv")
    shares = lax.axis_size("tp")
    features = inputs.shape[1]
    piece = features * shares // count
    window = (REACH + 2) * blocks
    bf16, f32 = jnp.bfloat16, jnp.float32

    pair = pl.pallas_call(
        pair_kernel,
        out_shape=pltpu.VMEM((tokens, 2 * width), bf16),
        in_specs=[pl.BlockSpec(memory_space=pltpu.HBM)] * 2,
        out_specs=pl.BlockSpec(memory_space=pltpu.VMEM),
        scratch_shapes=[pltpu.SemaphoreType.DMA((2,))],
        compiler_params=PARAMS,
    )(*far(keys, values))
    four = shifted(pair, 4)
    two = shifted(pair, 2)
    peer = swapped(pair, 1)
    peer_four = swapped(four, 1)
    peer_two = swapped(two, 1)

    keep, give = pl.pallas_call(
        functools.partial(transpose_kernel, piece),
        out_shape=[pltpu.VMEM((2, features // 4, tokens), bf16)] * 2,
        in_specs=[pl.BlockSpec(memory_space=pltpu.HBM)],
        out_specs=vmem(2),
        scratch_shapes=[
            pltpu.VMEM((tokens, features), bf16),
            pltpu.VMEM((features, tokens), bf16),
            pltpu.SemaphoreType.DMA((1,)),
        ],
        compiler_params=PARAMS,
    )(*far(inputs))
    chosen, queries, out_grad, log_sums = pl.pallas_call(
        fetch_kernel,
        out_shape=[pltpu.SMEM(chosen.shape, chosen.dtype)]
        + [pltpu.VMEM(v.shape, v.dtype) for v in (queries, out_grad, log_sums)],
        in_specs=[pl.BlockSpec(memory_space=pltpu.HBM)] * 4,
        out_specs=[pl.BlockSpec(memory_space=pltpu.SMEM)] + vmem(3),
        scratch_shapes=[pltpu.SemaphoreType.DMA((4,))],
        compiler_params=PARAMS,
    )(*far(chosen, queries, out_grad, log_sums))
    got = swapped(give, 1)
    own_factor, across = pl.pallas_call(
        join_kernel,
        out_shape=[pltpu.VMEM((features // 4, 2 * tokens), bf16)] * 2,
        in_specs=vmem(2),
        out_specs=vmem(2),
        compiler_params=PARAMS,
    )(*near(keep, got))
    own_factors, across_factors = [own_factor], [across]
    for step in range(1, shares):
        pairs = [(i, (i + step) % shares) for i in range(shares)]
        across_factors.append(lax.ppermute(across, "tp", pairs))
        own_factors.append(lax.ppermute(own_factor, "tp", pairs))

    queries, out_grad, log_sums = near(queries, out_grad, log_sums)
    chosen = pltpu.with_memory_space_constraint(chosen, pltpu.SMEM)
    value_acc, value_low, weights, key_values = pl.pallas_call(
        functools.partial(value_kernel, block),
        out_shape=[
            pltpu.VMEM((window, block, width), f32),
            pltpu.VMEM((4 * blocks, block, width), bf16),
            pltpu.VMEM((blocks, (slots + 1) * block, heads * block), f32),
            pltpu.VMEM((window, block, 2 * width), bf16),
        ],
        in_specs=[pl.BlockSpec(memory_space=pltpu.SMEM)] + vmem(9),
        out_specs=vmem(4),
        scratch_shapes=[pltpu.VMEM(((slots + 1) * block, width), bf16)],
        compiler_params=PARAMS,
    )(
        chosen,
        queries,
        out_grad,
        log_sums,
        *near(pair, two, four, peer, peer_two, peer_four),
    )
    query_grad, key_acc, key_low = pl.pallas_call(
        functools.partial(key_kernel, block),
        out_shape=[
            pltpu.VMEM(queries.shape, bf16),
            pltpu.VMEM((window, block, width), f32),
            pltpu.VMEM((4 * blocks, block, width), bf16),
        ],
        in_specs=[pl.BlockSpec(memory_space=pltpu.SMEM)] + vmem(4),
        out_specs=vmem(3),
        scratch_shapes=[pltpu.VMEM(((slots + 1) * block, width), bf16)] * 2,
        compiler_params=PARAMS,
    )(chosen, queries, out_grad, *near(weights, key_values))

    def gathered(acc, low, both):
        came = swapped(low, 1)
        own, send = pl.pallas_call(
            chip_sum_kernel,
            out_shape=[
                pltpu.VMEM((2 * blocks, block, width), f32),
                pltpu.VMEM((2 * blocks, block, width), bf16),
            ],
            in_specs=vmem(2),
            out_specs=vmem(2),
            compiler_params=PARAMS,
        )(*near(acc, came))
        back = returned(send)
        other = swapped(back, 1)
        return pl.pallas_call(
            total_kernel,
            out_shape=[pltpu.VMEM((2 * tokens, width), bf16)] * both
            + [pltpu.VMEM((tokens, width), bf16)],
            in_specs=vmem(3),
            out_specs=vmem(both + 1),
            compiler_params=PARAMS,
        )(*near(own, back, other))

    value_both, value_grad = gathered(value_acc, value_low, 1)
    (key_grad,) = gathered(key_acc, key_low, 0)

    pieces = count // 4

    def product(factors, dtype):
        return pl.pallas_call(
            functools.partial(product_kernel, shares),
            out_shape=pltpu.VMEM((pieces, piece, width), dtype),
            in_specs=vmem(1 + shares),
            out_specs=pl.BlockSpec(memory_space=pltpu.VMEM),
            compiler_params=PARAMS,
        )(*near(value_both, *factors))

    sent = product(across_factors, bf16)
    came = swapped(sent, 2)
    kept = product(own_factors, f32)
    stride = 4
    for radix in radices(pieces):
        kept, *sends = spread(kept, came, stride, radix)
        came = 0.0
        for s, send in enumerate(sends):
            came = came + turned(send, stride, radix, s + 1).astype(f32)
        stride *= radix
    weight_grad = (kept + came)[0]
    return (query_grad, key_grad, value_grad, weight_grad)


def solution(mesh):
    in_specs = (
        P("kv", "tp"),
        P("kv", "tp"),
        P("kv", "tp"),
        P("tp", "kv"),
        P("kv", "tp"),
        P("kv", "tp", None),
        P("kv", "tp"),
    )
    out_specs = (P("kv", "tp"), P("kv", "tp"), P("kv", "tp"), P("kv", "tp"))

    return jax.shard_map(shards, mesh=mesh, in_specs=in_specs, out_specs=out_specs, check_vma=False)
```

```python
import functools

import jax
import jax.numpy as jnp
from jax import lax
from jax.experimental import pallas as pl
from jax.experimental.pallas import tpu as pltpu
from jax.sharding import PartitionSpec as P


REACH = 4
LOG2E = 1.4426950408889634


PARAMS = pltpu.CompilerParams(vmem_limit_bytes=24 << 20)


def vmem(count):
    return [pl.BlockSpec(memory_space=pltpu.VMEM)] * count


def near(*values):
    return [pltpu.with_memory_space_constraint(v, pltpu.VMEM) for v in values]


def far(*values):
    return [pltpu.with_memory_space_constraint(v, pltpu.HBM) for v in values]


def shifted(value, steps):
    count = lax.axis_size("kv")
    return lax.ppermute(value, "kv", [(i, (i + steps) % count) for i in range(count)])


def returned(value):
    count = lax.axis_size("kv")
    moves = [(i, (i - (4 if i % 2 else 2)) % count) for i in range(count)]
    return lax.ppermute(value, "kv", moves)


def swapped(value, bit):
    count = lax.axis_size("kv")
    return lax.ppermute(value, "kv", [(i, i ^ bit) for i in range(count)])


def turned(value, stride, radix, steps):
    count = lax.axis_size("kv")
    pairs = []
    for i in range(count):
        digit = i // stride % radix
        target = (digit + steps) % radix if radix & (radix - 1) else digit ^ steps
        pairs.append((i, i + (target - digit) * stride))
    return lax.ppermute(value, "kv", pairs)


def places_of(chosen_ref, b, blocks):
    device = lax.axis_index("kv")
    odd = lax.rem(device, 2)
    first = (device - odd - REACH) * blocks
    listed = [chosen_ref[b, 0, s] for s in range(chosen_ref.shape[2])]
    return [c - first for c in listed] + [(REACH + odd) * blocks + b], listed


def stacked(ref, b, block, width):
    heads = ref.shape[1] // width
    here = pl.ds(b * block, block)
    return jnp.concatenate([ref[here, pl.ds(a * width, width)] for a in range(heads)], 0)


def value_kernel(
    block,
    chosen_ref,
    queries_ref,
    out_grad_ref,
    sums_ref,
    own_ref,
    two_ref,
    four_ref,
    peer_ref,
    peer_two_ref,
    peer_four_ref,
    value_acc,
    value_low_ref,
    weights_ref,
    window,
    key_rows,
):
    width = window.shape[2] // 2
    heads = queries_ref.shape[1] // width
    blocks = queries_ref.shape[0] // block
    slots = chosen_ref.shape[2]
    scaling = width ** (-0.5)
    device = lax.axis_index("kv")
    odd = lax.rem(device, 2)

    def place(position, ref):
        for b in range(blocks):
            window[position * blocks + b] = ref[pl.ds(b * block, block), :]

    for back, (mine, theirs) in enumerate(
        ((own_ref, peer_ref), (two_ref, peer_two_ref), (four_ref, peer_four_ref))
    ):
        place(REACH - 2 * back + odd, mine)
        place(REACH - 2 * back + 1 - odd, theirs)

    value_acc[...] = jnp.zeros_like(value_acc)
    rows = heads * block
    key_pos = lax.broadcasted_iota(jnp.int32, (block, rows), 0)
    query_pos = lax.rem(lax.broadcasted_iota(jnp.int32, (block, rows), 1), block)
    causal = key_pos <= query_pos
    for b in range(blocks):
        here = pl.ds(b * block, block)
        places, listed = places_of(chosen_ref, b, blocks)
        offsets = [jnp.where(c < device * blocks + b, 0.0, 1e30) for c in listed] + [0.0]
        for s in range(slots + 1):
            key_rows[pl.ds(s * block, block), :] = window[places[s], :, :width]
        q = stacked(queries_ref, b, block, width)
        g = stacked(out_grad_ref, b, block, width)
        sums = jnp.concatenate([sums_ref[pl.ds(a, 1), here] for a in range(heads)], 1) * LOG2E
        scores = lax.dot_general(
            key_rows[...], q, (((1,), (1,)), ((), ())), preferred_element_type=jnp.float32
        )
        low = []
        for s in range(slots + 1):
            part = slice(s * block, (s + 1) * block)
            weight = jnp.exp2(scores[part] * (scaling * LOG2E) - (sums + offsets[s]))
            if s == slots:
                weight = jnp.where(causal, weight, 0.0)
            weights_ref[b, pl.ds(s * block, block), :] = weight
            low.append(weight.astype(jnp.bfloat16))
        value_part = jnp.dot(jnp.concatenate(low, 0), g, preferred_element_type=jnp.float32)
        for s in range(slots + 1):
            value_acc[places[s]] += value_part[s * block : (s + 1) * block]
    hand_over(value_acc, value_low_ref)


def key_kernel(
    block,
    chosen_ref,
    queries_ref,
    out_grad_ref,
    weights_ref,
    window,
    query_grad_ref,
    key_acc,
    key_low_ref,
    key_rows,
    value_rows,
):
    width = window.shape[2] // 2
    heads = queries_ref.shape[1] // width
    blocks = queries_ref.shape[0] // block
    scaling = width ** (-0.5)
    key_acc[...] = jnp.zeros_like(key_acc)
    for b in range(blocks):
        places, _ = places_of(chosen_ref, b, blocks)
        for s, position in enumerate(places):
            key_rows[pl.ds(s * block, block), :] = window[position, :, :width]
            value_rows[pl.ds(s * block, block), :] = window[position, :, width:]
        q = stacked(queries_ref, b, block, width)
        g = stacked(out_grad_ref, b, block, width)
        grads = lax.dot_general(
            value_rows[...], g, (((1,), (1,)), ((), ())), preferred_element_type=jnp.float32
        )
        weights = weights_ref[b]
        delta = jnp.sum(weights * grads, 0, keepdims=True)
        score_grads = (weights * (grads - delta)).astype(jnp.bfloat16)
        key_part = jnp.dot(score_grads, q, preferred_element_type=jnp.float32) * scaling
        query_part = lax.dot_general(
            score_grads, key_rows[...], (((0,), (0,)), ((), ())), preferred_element_type=jnp.float32
        )
        for a in range(heads):
            query_grad_ref[pl.ds(b * block, block), pl.ds(a * width, width)] = (
                query_part[a * block : (a + 1) * block] * scaling
            ).astype(jnp.bfloat16)
        for s, position in enumerate(places):
            key_acc[position] += key_part[s * block : (s + 1) * block]
    hand_over(key_acc, key_low_ref)


def hand_over(acc_ref, low_ref):
    half = low_ref.shape[0] // 2
    odd = lax.rem(lax.axis_index("kv"), 2)
    low_ref[:half] = acc_ref[pl.ds(odd * half, half)].astype(jnp.bfloat16)
    low_ref[half:] = acc_ref[2 * half :].astype(jnp.bfloat16)


def chip_sum_kernel(mine_ref, came_ref, own_ref, send_ref):
    half = own_ref.shape[0]
    odd = lax.rem(lax.axis_index("kv"), 2)
    own_ref[...] = mine_ref[2 * half :] + came_ref[half:].astype(jnp.float32)
    total = mine_ref[pl.ds((1 - odd) * half, half)] + came_ref[:half].astype(jnp.float32)
    send_ref[...] = total.astype(jnp.bfloat16)


def total_kernel(own_ref, back_ref, other_ref, *refs):
    grad_ref = refs[-1]
    half = own_ref.shape[0] // 2
    odd = lax.rem(lax.axis_index("kv"), 2)

    def total(part):
        add = back_ref[part].astype(jnp.float32) + other_ref[part].astype(jnp.float32)
        return (own_ref[part] + add).astype(jnp.bfloat16)

    if len(refs) > 1:
        refs[0][...] = total(slice(None)).reshape(refs[0].shape)
    grad_ref[...] = total(pl.ds(odd * half, half)).reshape(grad_ref.shape)


def bring(pairs, done):
    copies = [pltpu.make_async_copy(a, b, done.at[i]) for i, (a, b) in enumerate(pairs)]
    for copy in copies:
        copy.start()
    for copy in copies:
        copy.wait()


def pair_kernel(keys_ref, values_ref, pair_ref, done):
    width = keys_ref.shape[1]
    left, right = pair_ref.at[:, pl.ds(0, width)], pair_ref.at[:, pl.ds(width, width)]
    bring([(keys_ref, left), (values_ref, right)], done)


def fetch_kernel(*refs):
    half = len(refs) // 2
    bring(list(zip(refs[:half], refs[half:-1])), refs[-1])


def transpose_kernel(piece, inputs_ref, keep_ref, give_ref, rows, turned_rows, done):
    bring([(inputs_ref, rows)], done)
    turned_rows[...] = rows[...].T
    corner = lax.rem(lax.axis_index("kv"), 4)
    for i in range(2):
        for out, owner in ((keep_ref, corner ^ (2 * i)), (give_ref, corner ^ (2 * i + 1))):
            for group in range(out.shape[1] // piece):
                out[i, pl.ds(group * piece, piece), :] = turned_rows[
                    pl.ds((4 * group + owner) * piece, piece), :
                ]


def join_kernel(keep_ref, got_ref, own_ref, across_ref):
    tokens = keep_ref.shape[2]
    odd = lax.rem(lax.axis_index("kv"), 2)
    for i, out in enumerate((own_ref, across_ref)):
        out[:, pl.ds(pl.multiple_of(odd * tokens, tokens), tokens)] = keep_ref[i]
        out[:, pl.ds(pl.multiple_of((1 - odd) * tokens, tokens), tokens)] = got_ref[i]


def partner(digit, step, radix):
    if radix & (radix - 1):
        return lax.rem(digit + step, radix)
    return digit ^ step


def product_kernel(shares, grads_ref, *refs):
    factors, out = refs[:shares], refs[shares]
    piece = out.shape[1]
    per_share = factors[0].shape[0] // piece
    part = lax.axis_index("tp")
    for step in range(shares):
        where = lax.rem(part + shares - step, shares)
        total = jnp.dot(factors[step][...], grads_ref[...], preferred_element_type=jnp.float32)
        for i in range(per_share):
            out[where * per_share + i] = total[i * piece : (i + 1) * piece].astype(out.dtype)


def spread_kernel(stride, radix, keep_ref, came_ref, *outs):
    mine_ref, sends = outs[0], outs[1:]
    digit = lax.rem(lax.axis_index("kv") // stride, radix)
    for i in range(mine_ref.shape[0]):
        at = radix * i + digit
        mine_ref[i] = keep_ref[at] + came_ref[at].astype(jnp.float32)
        for s, send in enumerate(sends):
            at = radix * i + partner(digit, s + 1, radix)
            send[i] = (keep_ref[at] + came_ref[at].astype(jnp.float32)).astype(jnp.bfloat16)


def spread(kept, came, stride, radix):
    shape = (kept.shape[0] // radix,) + kept.shape[1:]
    return pl.pallas_call(
        functools.partial(spread_kernel, stride, radix),
        out_shape=[pltpu.VMEM(shape, jnp.float32)] + [pltpu.VMEM(shape, jnp.bfloat16)] * (radix - 1),
        in_specs=vmem(2),
        out_specs=vmem(radix),
        compiler_params=PARAMS,
    )(*near(kept, came))


def radices(count):
    found = []
    for radix in (4, 3, 2):
        while count % radix == 0:
            found.append(radix)
            count //= radix
    if count > 1:
        found.append(count)
    return found


def shards(queries, keys, values, log_sums, out_grad, chosen, inputs):
    tokens, width = keys.shape
    blocks = chosen.shape[0]
    block = tokens // blocks
    heads = queries.shape[1] // width
    slots = chosen.shape[2]
    count = lax.axis_size("kv")
    shares = lax.axis_size("tp")
    features = inputs.shape[1]
    piece = features * shares // count
    window = (REACH + 2) * blocks
    bf16, f32 = jnp.bfloat16, jnp.float32

    pair = pl.pallas_call(
        pair_kernel,
        out_shape=pltpu.VMEM((tokens, 2 * width), bf16),
        in_specs=[pl.BlockSpec(memory_space=pltpu.HBM)] * 2,
        out_specs=pl.BlockSpec(memory_space=pltpu.VMEM),
        scratch_shapes=[pltpu.SemaphoreType.DMA((2,))],
        compiler_params=PARAMS,
    )(*far(keys, values))
    four = shifted(pair, 4)
    two = shifted(pair, 2)
    peer = swapped(pair, 1)
    peer_four = swapped(four, 1)
    peer_two = swapped(two, 1)

    keep, give = pl.pallas_call(
        functools.partial(transpose_kernel, piece),
        out_shape=[pltpu.VMEM((2, features // 4, tokens), bf16)] * 2,
        in_specs=[pl.BlockSpec(memory_space=pltpu.HBM)],
        out_specs=vmem(2),
        scratch_shapes=[
            pltpu.VMEM((tokens, features), bf16),
            pltpu.VMEM((features, tokens), bf16),
            pltpu.SemaphoreType.DMA((1,)),
        ],
        compiler_params=PARAMS,
    )(*far(inputs))
    chosen, queries, out_grad, log_sums = pl.pallas_call(
        fetch_kernel,
        out_shape=[pltpu.SMEM(chosen.shape, chosen.dtype)]
        + [pltpu.VMEM(v.shape, v.dtype) for v in (queries, out_grad, log_sums)],
        in_specs=[pl.BlockSpec(memory_space=pltpu.HBM)] * 4,
        out_specs=[pl.BlockSpec(memory_space=pltpu.SMEM)] + vmem(3),
        scratch_shapes=[pltpu.SemaphoreType.DMA((4,))],
        compiler_params=PARAMS,
    )(*far(chosen, queries, out_grad, log_sums))
    got = swapped(give, 1)
    own_factor, across = pl.pallas_call(
        join_kernel,
        out_shape=[pltpu.VMEM((features // 4, 2 * tokens), bf16)] * 2,
        in_specs=vmem(2),
        out_specs=vmem(2),
        compiler_params=PARAMS,
    )(*near(keep, got))
    own_factors, across_factors = [own_factor], [across]
    for step in range(1, shares):
        pairs = [(i, (i + step) % shares) for i in range(shares)]
        across_factors.append(lax.ppermute(across, "tp", pairs))
        own_factors.append(lax.ppermute(own_factor, "tp", pairs))

    queries, out_grad, log_sums = near(queries, out_grad, log_sums)
    chosen = pltpu.with_memory_space_constraint(chosen, pltpu.SMEM)
    value_acc, value_low, weights, key_values = pl.pallas_call(
        functools.partial(value_kernel, block),
        out_shape=[
            pltpu.VMEM((window, block, width), f32),
            pltpu.VMEM((4 * blocks, block, width), bf16),
            pltpu.VMEM((blocks, (slots + 1) * block, heads * block), f32),
            pltpu.VMEM((window, block, 2 * width), bf16),
        ],
        in_specs=[pl.BlockSpec(memory_space=pltpu.SMEM)] + vmem(9),
        out_specs=vmem(4),
        scratch_shapes=[pltpu.VMEM(((slots + 1) * block, width), bf16)],
        compiler_params=PARAMS,
    )(
        chosen,
        queries,
        out_grad,
        log_sums,
        *near(pair, two, four, peer, peer_two, peer_four),
    )
    query_grad, key_acc, key_low = pl.pallas_call(
        functools.partial(key_kernel, block),
        out_shape=[
            pltpu.VMEM(queries.shape, bf16),
            pltpu.VMEM((window, block, width), f32),
            pltpu.VMEM((4 * blocks, block, width), bf16),
        ],
        in_specs=[pl.BlockSpec(memory_space=pltpu.SMEM)] + vmem(4),
        out_specs=vmem(3),
        scratch_shapes=[pltpu.VMEM(((slots + 1) * block, width), bf16)] * 2,
        compiler_params=PARAMS,
    )(chosen, queries, out_grad, *near(weights, key_values))

    def gathered(acc, low, both):
        came = swapped(low, 1)
        own, send = pl.pallas_call(
            chip_sum_kernel,
            out_shape=[
                pltpu.VMEM((2 * blocks, block, width), f32),
                pltpu.VMEM((2 * blocks, block, width), bf16),
            ],
            in_specs=vmem(2),
            out_specs=vmem(2),
            compiler_params=PARAMS,
        )(*near(acc, came))
        back = returned(send)
        other = swapped(back, 1)
        return pl.pallas_call(
            total_kernel,
            out_shape=[pltpu.VMEM((2 * tokens, width), bf16)] * both
            + [pltpu.VMEM((tokens, width), bf16) if both else jax.ShapeDtypeStruct((tokens, width), bf16)],
            in_specs=vmem(3),
            out_specs=vmem(both + 1),
            compiler_params=PARAMS,
        )(*near(own, back, other))

    value_both, value_grad = gathered(value_acc, value_low, 1)
    (key_grad,) = gathered(key_acc, key_low, 0)

    query_grad, value_grad = pl.pallas_call(
        fetch_kernel,
        out_shape=[jax.ShapeDtypeStruct(v.shape, v.dtype) for v in (query_grad, value_grad)],
        in_specs=vmem(2),
        out_specs=[pl.BlockSpec(memory_space=pltpu.HBM)] * 2,
        scratch_shapes=[pltpu.SemaphoreType.DMA((2,))],
        compiler_params=PARAMS,
    )(*near(query_grad, value_grad))

    pieces = count // 4

    def product(factors, dtype):
        return pl.pallas_call(
            functools.partial(product_kernel, shares),
            out_shape=pltpu.VMEM((pieces, piece, width), dtype),
            in_specs=vmem(1 + shares),
            out_specs=pl.BlockSpec(memory_space=pltpu.VMEM),
            compiler_params=PARAMS,
        )(*near(value_both, *factors))

    sent = product(across_factors, bf16)
    came = swapped(sent, 2)
    kept = product(own_factors, f32)
    stride = 4
    for radix in radices(pieces):
        kept, *sends = spread(kept, came, stride, radix)
        came = 0.0
        for s, send in enumerate(sends):
            came = came + turned(send, stride, radix, s + 1).astype(f32)
        stride *= radix
    weight_grad = (kept + came)[0]
    return (query_grad, key_grad, value_grad, weight_grad)


def solution(mesh):
    in_specs = (
        P("kv", "tp"),
        P("kv", "tp"),
        P("kv", "tp"),
        P("tp", "kv"),
        P("kv", "tp"),
        P("kv", "tp", None),
        P("kv", "tp"),
    )
    out_specs = (P("kv", "tp"), P("kv", "tp"), P("kv", "tp"), P("kv", "tp"))

    return jax.shard_map(shards, mesh=mesh, in_specs=in_specs, out_specs=out_specs, check_vma=False)
```
